256 devices in a mesh: sp: 64 (over z, y, core), tp: 4 (over x).
Axes of the slice: x: 4, y: 4, z: 8, core: 2. Of those that a mesh axis runs over, the one named last changes fastest.
Arguments:
- tokens: bfloat16 [16384, 2048], P(('sp', 'tp')), may hold values from -6 to 6
- norm_gain: float32 [2048], replicated, may hold values from 0.1 to 6, as said below
- query_weight: bfloat16 [2048, 16, 128], P(None, 'tp'), may hold values from -0.21875 to 0.21875
- key_weight: bfloat16 [2048, 4, 128], P(None, 'tp'), may hold values from -0.125 to 0.125
- value_weight: bfloat16 [2048, 4, 128], P(None, 'tp'), may hold values from -0.125 to 0.125
- mix_lambda: float32 [16], P('tp'), may hold values from 0.3 to 0.8
- head_gain: float32 [128], replicated, may hold values from 0.1 to 1.9
- pool_weight: bfloat16 [2048, 4, 512], P(None, 'tp'), may hold values from -0.125 to 0.125
- pool_mix: bfloat16 [4, 512, 512], P('tp'), may hold values from -0.25 to 0.25
- pool_scale: float32 [4, 512], P('tp'), may hold values from 0.1 to 1.9
- gate_weight: bfloat16 [2048, 2, 2048], P(None, None, 'tp'), may hold values from -0.125 to 0.125
- out_weight: bfloat16 [2048, 2048], P('tp'), may hold values from -0.125 to 0.125
Outputs:
- mixed: bfloat16 [16384, 2048], P(('sp', 'tp'))
- log_sums: float32 [2, 16, 16384], P(None, 'tp', 'sp')
The draws below stay inside these ranges and needn't reach their ends.
Inputs may be any that keep to these rules, and one draw needn't show every extreme that they name: `norm_gain`: positive.
All inputs are finite; a program needn't handle non-finite values.
Results may differ from the reference program's by a relative error of at most 0.013.
Values may be sent and summed in bfloat16 or wider, within the bound.
No kernel may reach another device: no remote copies, remote signals or barrier semaphores. Data moves between devices by JAX's collectives and lax.ppermute only.
A program may use at most 128 MiB of HBM per device.

```python
import math
import jax
import jax.numpy as jnp
from jax import lax

D = 2048
HEADS = 16
HD = 64
DV = 128
KV_HEADS = 4
GROUPS = 4
GW = 512
WINDOW = 16
TOKENS = 16384
N_TP = 4


def draw_norm_gain(key, part):
    return 1.0 + 0.18 * jnp.clip(jax.random.normal(key, (D,), jnp.float32), -5.0, 5.0)


def block_levels(stream_key, extent, shards, least, largest):
    factor_of = 1.0
    for dim, parts in shards:
        draws = jax.random.uniform(jax.random.fold_in(jax.random.fold_in(stream_key, 6), dim), (parts,), jnp.float32, least / len(shards), largest / len(shards))
        factor_of = factor_of * jnp.repeat(jnp.exp(draws), extent[dim] // parts).reshape((-1,) + (1,) * (len(extent) - 1 - dim))
    return factor_of


def bell_draw(own_key, dims, width, most, cuts=(), held_as=jnp.bfloat16):
    values = width * jax.random.normal(own_key, dims, jnp.float32)
    if cuts:
        values = values * block_levels(own_key, dims, cuts, -0.22, 0.18)
    return jnp.clip(values, -most, most).astype(held_as)


def setup_inputs(seed: int = 0) -> dict:
    key_list = jax.random.split(jax.random.key(seed), 13)
    return {
        "tokens": bell_draw(key_list[0], (TOKENS, D), 1.0, 6.0, ((0, 256),)),
        "norm_gain": draw_norm_gain(jax.random.fold_in(key_list[12], 71), 0),
        "query_weight": bell_draw(key_list[2], (D, HEADS, 2 * HD), (D // 3) ** -0.5, 0.21875, ((1, 4),)),
        "key_weight": bell_draw(key_list[3], (D, KV_HEADS, 2 * HD), D ** -0.5, 0.125, ((1, 4),)),
        "value_weight": bell_draw(key_list[4], (D, KV_HEADS, DV), D ** -0.5, 0.125, ((1, 4),)),
        "mix_lambda": jnp.clip(0.3 + 0.5 * jax.random.uniform(key_list[5], (HEADS,), jnp.float32) ** block_levels(key_list[5], (HEADS,), ((0, 4),), -0.2, 0.2), 0.3, 0.8),
        "head_gain": jnp.clip(1.0 + 0.18 * jax.random.normal(key_list[6], (DV,), jnp.float32), 0.1, 1.9),
        "pool_weight": bell_draw(key_list[7], (D, GROUPS, GW), D ** -0.5, 0.125, ((1, 4),)),
        "pool_mix": bell_draw(key_list[8], (GROUPS, GW, GW), GW ** -0.5, 0.25, ((0, 4),)),
        "pool_scale": jnp.clip(1.0 + 0.18 * jax.random.normal(key_list[9], (GROUPS, GW), jnp.float32), 0.1, 1.9),
        "gate_weight": bell_draw(key_list[10], (D, 2, D), D ** -0.5, 0.125, ((2, 4),)),
        "out_weight": bell_draw(key_list[11], (D, D), D ** -0.5, 0.125, ((0, 4),)),
    }


NORM_EPS = 1e-06

def reference(tokens, norm_gain, query_weight, key_weight, value_weight, mix_lambda, head_gain, pool_weight, pool_mix, pool_scale, gate_weight, out_weight):
    inputs = tokens.astype(jnp.float32)
    normed = (inputs * lax.rsqrt(lax.optimization_barrier(jnp.mean(inputs * inputs, axis=1, keepdims=True)) + NORM_EPS) * norm_gain).astype(jnp.bfloat16)

    def project(weight):
        return jnp.dot(normed, weight.reshape(D, -1), preferred_element_type=jnp.float32).astype(jnp.bfloat16)
    queries = project(query_weight).reshape(TOKENS, HEADS, 2, HD)
    keys_all = project(key_weight).reshape(TOKENS, KV_HEADS, 2, HD)
    values_all = project(value_weight).reshape(TOKENS, KV_HEADS, DV)
    pool_in = project(pool_weight).reshape(TOKENS, GROUPS, GW)
    gate_pre = project(gate_weight).reshape(TOKENS, 2, D)
    group_size = HEADS // KV_HEADS
    block_rows = math.gcd(TOKENS, 1024)
    positions = jnp.arange(TOKENS, dtype=jnp.int32)
    score_scale = HD ** (-0.5)

    def one_head(head_index):
        kv_index = head_index // group_size
        head_queries = lax.dynamic_index_in_dim(queries, head_index, 1, keepdims=False).astype(jnp.float32)
        head_keys = lax.dynamic_index_in_dim(keys_all, kv_index, 1, keepdims=False).astype(jnp.float32)
        head_values = lax.dynamic_index_in_dim(values_all, kv_index, 1, keepdims=False)
        weight_lambda = lax.dynamic_index_in_dim(mix_lambda, head_index, 0, keepdims=False)

        def one_block(block_index):
            first_row = block_index * block_rows
            block_queries = lax.dynamic_slice_in_dim(head_queries, first_row, block_rows, 0)
            query_pos = first_row + jnp.arange(block_rows, dtype=jnp.int32)
            scores = jnp.einsum('qmd,kmd->mqk', block_queries, head_keys) * score_scale
            causal = positions[None, None, :] <= query_pos[None, :, None]
            masked = jnp.where(causal, scores, -jnp.inf)
            row_top = lax.optimization_barrier(jnp.max(masked, axis=2, keepdims=True))
            probs = jnp.exp(masked - row_top)
            row_sum = lax.optimization_barrier(jnp.sum(probs, axis=2, keepdims=True))
            log_total = row_top + jnp.log(row_sum)
            probs_low = probs.astype(jnp.bfloat16)
            first_map = jnp.dot(probs_low[0], head_values, preferred_element_type=jnp.float32)
            second_map = jnp.dot(probs_low[1], head_values, preferred_element_type=jnp.float32)
            block_out = first_map / row_sum[0] - weight_lambda * (second_map / row_sum[1])
            return (block_out, log_total[:, :, 0])
        outs, logs = lax.map(one_block, jnp.arange(TOKENS // block_rows, dtype=jnp.int32))
        return (outs.reshape(TOKENS, DV), jnp.transpose(logs, (1, 0, 2)).reshape(2, TOKENS))
    head_outs, head_logs = lax.map(one_head, jnp.arange(HEADS, dtype=jnp.int32))
    normed_heads = head_outs * lax.rsqrt(lax.optimization_barrier(jnp.mean(head_outs * head_outs, axis=2, keepdims=True)) + NORM_EPS) * head_gain
    attended = jnp.transpose(normed_heads, (1, 0, 2)).reshape(TOKENS, D)
    extended = jnp.concatenate([jnp.zeros((WINDOW, GROUPS, GW), jnp.float32), pool_in.astype(jnp.float32)], axis=0)
    group_parts = []
    for group_index in range(GROUPS):
        window_span = 2 ** (group_index + 1)
        window_sum = jnp.zeros((TOKENS, GW), jnp.float32)
        for back_rows in range(window_span):
            window_sum = window_sum + extended[WINDOW - back_rows:WINDOW - back_rows + TOKENS, group_index]
        counts = jnp.minimum(positions + 1, window_span).astype(jnp.float32)
        means = window_sum / counts[:, None]
        pooled = (means - pool_in[:, group_index].astype(jnp.float32)).astype(jnp.bfloat16)
        group_parts.append(jnp.dot(pooled, pool_mix[group_index], preferred_element_type=jnp.float32) * pool_scale[group_index])
    pool_out = jnp.concatenate(group_parts, axis=1)
    merged = (jax.nn.sigmoid(gate_pre[:, 0].astype(jnp.float32)) * attended + jax.nn.sigmoid(gate_pre[:, 1].astype(jnp.float32)) * pool_out).astype(jnp.bfloat16)
    block_cols = D // N_TP
    out_total = jnp.zeros((TOKENS, D), jnp.float32)
    for part_index in range(N_TP):
        partial_out = jnp.dot(merged[:, part_index * block_cols:(part_index + 1) * block_cols], out_weight[part_index * block_cols:(part_index + 1) * block_cols], preferred_element_type=jnp.float32).astype(jnp.bfloat16)
        out_total = out_total + lax.optimization_barrier(partial_out).astype(jnp.float32)
    return (out_total.astype(jnp.bfloat16), jnp.transpose(head_logs, (1, 0, 2)))
```

```python
import functools
import math

import jax
import jax.numpy as jnp
from jax import lax
from jax.experimental import pallas as pl
from jax.experimental.pallas import tpu as pltpu
from jax.sharding import Mesh
from jax.sharding import PartitionSpec as P

NORM_EPS = 1e-06
WINDOW = 16
ROWS = 256
HALF = 128
MAPS = 8
ST = 152
NEG = -1e30
LIMIT = 64.0
LOG2E = math.log2(math.e)
VMEM = pl.BlockSpec(memory_space=pltpu.VMEM)
SMEM = pl.BlockSpec(memory_space=pltpu.SMEM)
F32 = jnp.float32
BF16 = jnp.bfloat16


def vmem(mib):
    return pltpu.CompilerParams(vmem_limit_bytes=mib << 20)


def ring(size, step):
    return [(i, (i + step) % size) for i in range(size)]


def dot(a, b):
    return jnp.dot(a, b, preferred_element_type=F32)


def with_ones(v0, v1):
    values = jnp.concatenate([v0, v1], axis=1)
    return jnp.concatenate([values, jnp.ones((16, values.shape[1]), BF16)], axis=0)


def first_kernel(place_ref, kv_ref, oth_kv_ref, q_ref, own_ref, oth_ref):
    keys = jnp.concatenate([kv_ref[0, 0, :, :HALF], kv_ref[1, 0, :, :HALF]], axis=0)
    oth_keys = jnp.concatenate([oth_kv_ref[0, 0, :, :HALF], oth_kv_ref[1, 0, :, :HALF]], axis=0)
    values = with_ones(kv_ref[0, 0, :, HALF:], kv_ref[1, 0, :, HALF:])
    row = lax.broadcasted_iota(jnp.int32, (ROWS, ROWS), 0)
    col = lax.broadcasted_iota(jnp.int32, (ROWS, ROWS), 1)
    diagonal = row <= col
    for i in range(MAPS):
        q_own, q_oth = q_ref[i, :, :ROWS], q_ref[i, :, ROWS:]
        s = jnp.where(diagonal, dot(keys, q_own), NEG)
        top = jnp.max(s, axis=0, keepdims=True)
        p = jnp.exp2(s - top).astype(BF16)
        own_ref[i, 0:144] = dot(values, p)
        own_ref[i, 144:152] = jnp.broadcast_to(top, (8, ROWS))
        top = jnp.max(jnp.where(diagonal, dot(oth_keys, q_oth), NEG), axis=0, keepdims=True)
        oth_ref[i, 144:152] = jnp.broadcast_to(top, (8, ROWS))
        oth_ref[i, 0:144] = jnp.zeros((144, ROWS), F32)

    @pl.when(place_ref[2] == 0)
    def _():
        for i in range(MAPS):
            before = oth_ref[i, 144:145]
            s = dot(keys, q_ref[i, :, ROWS:])
            top = jnp.maximum(before, jnp.max(s, axis=0, keepdims=True))
            p = jnp.exp2(s - top).astype(BF16)
            oth_ref[i, 0:144] = dot(values, p)
            oth_ref[i, 144:152] = jnp.broadcast_to(top, (8, ROWS))


def chunk_kernel(plan, n_in, *refs):
    place_ref, q_ref = refs[0], refs[1]
    ins = refs[2 : 2 + n_in]
    own_in, oth_in, own_ref, oth_ref, keys_ref, values_ref, p_a, p_b, over_ref, list_ref = refs[2 + n_in :]
    probs = (p_a, p_b)
    z, y = place_ref[0], place_ref[1]
    visible = jnp.int32(0)
    at = 0
    for _, dy, planes in plan:
        for dz in planes:
            sees = ((z + dz) & 7) * 4 + ((y + dy) & 3) < z * 4 + y
            list_ref[visible] = at
            visible = visible + sees.astype(jnp.int32)
            at += 1

    def fetch(which, slot):
        at = 0
        rows = slice(slot * ROWS, slot * ROWS + HALF), slice(slot * ROWS + HALF, slot * ROWS + ROWS)
        for pair, _, planes in plan:
            count = len(planes)

            @pl.when((which >= at) & (which < at + count))
            def _(pair=pair, at=at):
                b = which - at
                for half in range(2):
                    source = ins[pair[half]].at[b] if isinstance(pair, tuple) else ins[pair].at[half, b]
                    keys_ref[rows[half]] = source[:, :HALF]
                    values_ref[0:HALF, rows[half]] = source[:, HALF:]
            at += count

    own_ref[...] = own_in[...]
    oth_ref[...] = oth_in[...]

    @pl.when(visible > 0)
    def _():
        over_ref[...] = jnp.full(over_ref.shape, NEG, F32)
        values_ref[HALF:144] = jnp.ones((16, 2 * ROWS), BF16)

        def two_blocks(t, carry):
            fetch(list_ref[2 * t], 0)
            second = 2 * t + 1 < visible
            fetch(list_ref[jnp.minimum(2 * t + 1, visible - 1)], 1)

            @pl.when(jnp.logical_not(second))
            def _():
                values_ref[:, ROWS:] = jnp.zeros((144, ROWS), BF16)

            keys, values = keys_ref[...], values_ref[...]

            def scores(i):
                top = jnp.concatenate([own_ref[i, 144:145], oth_ref[i, 144:145]], axis=1)
                s = dot(keys, q_ref[i]) - top
                over_ref[i] = jnp.maximum(over_ref[i], jnp.max(s.reshape(-1, 8, 2 * ROWS), axis=0))
                probs[i % 2][...] = jnp.exp2(s).astype(BF16)

            scores(0)
            for i in range(MAPS):
                if i + 1 < MAPS:
                    scores(i + 1)
                out = dot(values, probs[i % 2][...])
                own_ref[i, 0:144] = own_ref[i, 0:144] + out[:, :ROWS]
                oth_ref[i, 0:144] = oth_ref[i, 0:144] + out[:, ROWS:]
            return carry

        lax.fori_loop(0, (visible + 1) // 2, two_blocks, 0)

        @pl.when(jnp.logical_not(jnp.max(over_ref[...]) <= LIMIT))
        def _():
            own_ref[...] = own_in[...]
            oth_ref[...] = oth_in[...]
            values_ref[HALF:144] = jnp.ones((16, 2 * ROWS), BF16)

            def one_block(t, carry):
                fetch(list_ref[t], 0)

                def one_map(i, carry):
                    before = jnp.concatenate([own_ref[i, 144:145], oth_ref[i, 144:145]], axis=1)
                    s = dot(keys_ref[:ROWS], q_ref[i])
                    top = jnp.maximum(before, jnp.max(s, axis=0, keepdims=True))
                    scale = jnp.exp2(before - top)
                    out = dot(values_ref[:, :ROWS], jnp.exp2(s - top).astype(BF16))
                    top8 = jnp.broadcast_to(top, (8, 2 * ROWS))
                    own_ref[i, 0:144] = own_ref[i, 0:144] * scale[:, :ROWS] + out[:, :ROWS]
                    oth_ref[i, 0:144] = oth_ref[i, 0:144] * scale[:, ROWS:] + out[:, ROWS:]
                    own_ref[i, 144:152] = top8[:, :ROWS]
                    oth_ref[i, 144:152] = top8[:, ROWS:]
                    return carry

                return lax.fori_loop(0, MAPS, one_map, carry)

            lax.fori_loop(0, visible, one_block, 0)


STATE = (pltpu.VMEM((MAPS, ST, ROWS), F32), pltpu.VMEM((MAPS, ST, ROWS), F32))


def in_vmem(array):
    return pltpu.with_memory_space_constraint(array, pltpu.VMEM)


def attend_chunk(place, q, state, plan, arrays, name):
    n = len(arrays)
    blocks = sum(len(planes) for _, _, planes in plan)
    return pl.pallas_call(
        functools.partial(chunk_kernel, plan, n),
        out_shape=STATE,
        in_specs=[SMEM, VMEM] + [VMEM] * n + [VMEM, VMEM],
        out_specs=(VMEM, VMEM),
        scratch_shapes=[
            pltpu.VMEM((2 * ROWS, HALF), BF16),
            pltpu.VMEM((144, 2 * ROWS), BF16),
            pltpu.VMEM((2 * ROWS, 2 * ROWS), BF16),
            pltpu.VMEM((2 * ROWS, 2 * ROWS), BF16),
            pltpu.VMEM((MAPS, 8, 2 * ROWS), F32),
            pltpu.SMEM((blocks + 1,), jnp.int32),
        ],
        cost_estimate=pl.CostEstimate(
            flops=blocks * MAPS * 2 * 256 * 512 * 512, transcendentals=blocks * MAPS * 256 * 512, bytes_accessed=1 << 20
        ),
        compiler_params=vmem(20),
        name=name,
    )(place, in_vmem(q), *arrays, in_vmem(state[0]), in_vmem(state[1]))


def pool_kernel(place_ref, pool_ref, rim_ref, gate_ref, mix_ref, scale_ref, keep_ref, part_ref):
    span = jnp.left_shift(jnp.int32(2), place_ref[3])
    start = ((place_ref[0] * 4 + place_ref[1]) * 2 + place_ref[2]) * ROWS
    now = pool_ref[...].astype(F32)
    sums = jnp.concatenate([rim_ref[...].astype(F32), now], axis=0)
    rows = WINDOW + ROWS
    picked = jnp.zeros((ROWS, now.shape[1]), F32)
    for width in (1, 2, 4, 8):
        sums = sums + jnp.concatenate([jnp.zeros((width, now.shape[1]), F32), sums[: rows - width]], axis=0)
        picked = jnp.where(span == 2 * width, sums[WINDOW:], picked)
    position = start + lax.broadcasted_iota(jnp.int32, (ROWS, 1), 0)
    counts = jnp.minimum(position + 1, span).astype(F32)
    pooled = (picked / counts - now).astype(BF16)
    mixed = dot(pooled, mix_ref[...]) * scale_ref[...]
    width = now.shape[1]
    keep_ref[...] = jax.nn.sigmoid(gate_ref[:, :width].astype(F32))
    part_ref[...] = jax.nn.sigmoid(gate_ref[:, width:].astype(F32)) * mixed


def finish_kernel(lam_ref, a_ref, b_ref, gain_ref, keep_ref, part_ref, w_ref, out_ref, log_ref, merged_ref):
    for h in range(MAPS // 2):
        maps = []
        for m in range(2):
            i = 2 * h + m
            top_a, top_b = a_ref[i, 144:145], b_ref[i, 144:145]
            top = jnp.maximum(top_a, top_b)
            wa, wb = jnp.exp2(top_a - top), jnp.exp2(top_b - top)
            total = a_ref[i, 128:129] * wa + b_ref[i, 128:129] * wb
            log_ref[i : i + 1, :] = (top + jnp.log2(total)) * (1.0 / LOG2E)
            maps.append((a_ref[i, 0:128] * wa + b_ref[i, 0:128] * wb) / total)
        head = maps[0] - lam_ref[h] * maps[1]
        head = head * lax.rsqrt(jnp.mean(head * head, axis=0, keepdims=True) + NORM_EPS)
        cols = slice(h * 128, h * 128 + 128)
        attended = head.T * gain_ref[...]
        merged_ref[:, cols] = (keep_ref[:, cols] * attended + part_ref[:, cols]).astype(BF16)
    out_ref[...] = dot(merged_ref[...], w_ref[...]).astype(BF16)


def local(tokens, norm_gain, query_weight, key_weight, value_weight, mix_lambda, head_gain, pool_weight, pool_mix, pool_scale, gate_weight, out_weight):
    width = tokens.shape[1]
    z, y, c = lax.axis_index("z"), lax.axis_index("y"), lax.axis_index("c")
    place = jnp.stack([z, y, c, lax.axis_index("x")])
    pieces = lax.all_to_all(jnp.broadcast_to(tokens[None], (4, *tokens.shape)), "x", 0, 0, tiled=True)
    gate_w, query_w = gate_weight.reshape(width, -1), query_weight.reshape(width, -1)
    pieces, gate_w, query_w = lax.optimization_barrier((pieces, gate_w, query_w))
    inputs = pieces.reshape(ROWS, width).astype(F32)
    normed = (inputs * lax.rsqrt(jnp.mean(inputs * inputs, axis=1, keepdims=True) + NORM_EPS) * norm_gain).astype(BF16)

    def project(weight):
        return dot(normed, weight.reshape(width, -1)).astype(BF16)

    keys = project(key_weight)
    values_t = lax.dot_general(value_weight.reshape(width, 128), normed, (((0,), (1,)), ((), ())), preferred_element_type=F32).astype(BF16)
    kv = jnp.concatenate(
        [keys.reshape(2, 1, HALF, HALF), jnp.transpose(values_t.reshape(HALF, 2, HALF), (1, 0, 2))[:, None]], axis=3
    )
    up, down = [kv], [kv]
    for k in range(4):
        up.append(lax.ppermute(up[-1], "z", ring(8, 1)))
        if k < 3:
            down.append(lax.ppermute(down[-1], "z", ring(8, -1)))
    near = jnp.concatenate([kv, up[1], down[1]], axis=1)
    far = jnp.concatenate([up[2], up[3], up[4], down[2], down[3]], axis=1)
    near_at, far_at = (0, -1, 1), (-2, -3, -4, 2, 3)

    def around_y(group):
        low = lax.ppermute(group, "y", ring(4, 1))
        high = lax.ppermute(group, "y", ring(4, -1))
        a = lax.ppermute(low[0], "y", ring(4, 1))
        b = lax.ppermute(high[1], "y", ring(4, -1))
        return low, high, a, b

    scale = (query_weight.shape[2] // 2) ** -0.5 * LOG2E
    q_own = (
        lax.dot_general(query_w, normed, (((0,), (1,)), ((), ())), preferred_element_type=F32) * scale
    ).astype(BF16)
    q_oth = lax.ppermute(q_own, "c", [(0, 1), (1, 0)])
    kv_oth = lax.ppermute(kv, "c", [(0, 1), (1, 0)])
    q = jnp.concatenate([q_own, q_oth], axis=1).reshape(4, 2, 64, 2 * ROWS)
    zero = jnp.zeros((4, 64, 2 * ROWS), BF16)
    q = jnp.stack([jnp.concatenate([q[:, 0], zero], axis=1), jnp.concatenate([zero, q[:, 1]], axis=1)], axis=1)
    q = q.reshape(MAPS, 128, 2 * ROWS)

    pool_in = project(pool_weight)
    gate_pre = project(gate_w)
    rim = lax.ppermute(pool_in[ROWS - WINDOW :], ("z", "y", "c"), [(i, i + 1) for i in range(63)])
    part_shape = jax.ShapeDtypeStruct((ROWS, 512), F32)
    keep, part = pl.pallas_call(
        pool_kernel,
        out_shape=(part_shape, part_shape),
        in_specs=[SMEM] + [VMEM] * 5,
        out_specs=(VMEM, VMEM),
        compiler_params=vmem(16),
        name="pool",
    )(place, pool_in, rim, gate_pre, pool_mix[0], pool_scale)

    state = pl.pallas_call(
        first_kernel, out_shape=STATE, in_specs=[SMEM, VMEM, VMEM, VMEM], out_specs=(VMEM, VMEM), compiler_params=vmem(16), name="first"
    )(place, kv, kv_oth, in_vmem(q))
    state, keep, part = lax.optimization_barrier((state, keep, part))
    state = attend_chunk(place, q, state, ((0, 0, (-1,)), (1, 0, (1,))), (up[1], down[1]), "z_near")
    state = attend_chunk(place, q, state, ((0, 0, far_at),), (far,), "z_far")
    for group, at, name in ((near, near_at, "near"), (far, far_at, "far")):
        low, high, a, b = around_y(group)
        state = attend_chunk(place, q, state, ((0, -1, at), (1, 1, at)), (low, high), "y_" + name)
        state = attend_chunk(place, q, state, (((0, 1), 2, at),), (a, b), "d_" + name)
    other = lax.ppermute(state[1], "c", [(0, 1), (1, 0)])
    out, logs = pl.pallas_call(
        finish_kernel,
        out_shape=(jax.ShapeDtypeStruct((ROWS, width), BF16), jax.ShapeDtypeStruct((MAPS, ROWS), F32)),
        in_specs=[SMEM] + [VMEM] * 6,
        out_specs=(VMEM, VMEM),
        scratch_shapes=[pltpu.VMEM((ROWS, 512), BF16)],
        compiler_params=vmem(24),
        name="finish",
    )(mix_lambda, state[0], other, head_gain[None], keep, part, out_weight)
    shares = lax.all_to_all(out.reshape(4, 64, width), "x", 0, 0, tiled=True)
    mixed = jnp.sum(shares.astype(F32), axis=0).astype(BF16)
    return mixed, jnp.transpose(logs.reshape(4, 2, ROWS), (1, 0, 2))


def solution(mesh):
    fine = Mesh(mesh.devices.reshape(8, 4, 2, 4), ("z", "y", "c", "x"))
    sp = ("z", "y", "c")
    in_specs = (
        P((*sp, "x"), None),
        P(),
        P(None, "x", None),
        P(None, "x", None),
        P(None, "x", None),
        P("x"),
        P(),
        P(None, "x", None),
        P("x", None, None),
        P("x", None),
        P(None, None, "x"),
        P("x", None),
    )
    out_specs = (P((*sp, "x"), None), P(None, "x", sp))
    return jax.shard_map(local, mesh=fine, in_specs=in_specs, out_specs=out_specs, check_vma=False)
```

```python
import functools
import math

import jax
import jax.numpy as jnp
from jax import lax
from jax.experimental import pallas as pl
from jax.experimental.pallas import tpu as pltpu
from jax.sharding import Mesh
from jax.sharding import PartitionSpec as P

NORM_EPS = 1e-06
WINDOW = 16
ROWS = 256
HALF = 128
MAPS = 8
ST = 152
NEG = -1e30
LIMIT = 64.0
LOG2E = math.log2(math.e)
VMEM = pl.BlockSpec(memory_space=pltpu.VMEM)
SMEM = pl.BlockSpec(memory_space=pltpu.SMEM)
F32 = jnp.float32
BF16 = jnp.bfloat16


def vmem(mib):
    return pltpu.CompilerParams(vmem_limit_bytes=mib << 20)


def ring(size, step):
    return [(i, (i + step) % size) for i in range(size)]


def dot(a, b):
    return jnp.dot(a, b, preferred_element_type=F32)


def with_ones(v0, v1):
    values = jnp.concatenate([v0, v1], axis=1)
    return jnp.concatenate([values, jnp.ones((16, values.shape[1]), BF16)], axis=0)


def first_kernel(place_ref, kv_ref, oth_kv_ref, q_ref, own_ref, oth_ref):
    keys = jnp.concatenate([kv_ref[0, 0, :, :HALF], kv_ref[0, 1, :, :HALF]], axis=0)
    oth_keys = jnp.concatenate([oth_kv_ref[0, 0, :, :HALF], oth_kv_ref[0, 1, :, :HALF]], axis=0)
    values = with_ones(kv_ref[0, 0, :, HALF:], kv_ref[0, 1, :, HALF:])
    row = lax.broadcasted_iota(jnp.int32, (ROWS, ROWS), 0)
    col = lax.broadcasted_iota(jnp.int32, (ROWS, ROWS), 1)
    diagonal = row <= col
    both = place_ref[2] == 0

    def one_map(i, carry):
        q_own, q_oth = q_ref[i, :, :ROWS], q_ref[i, :, ROWS:]
        s = jnp.where(diagonal, dot(keys, q_own), NEG)
        top = jnp.max(s, axis=0, keepdims=True)
        p = jnp.exp2(s - top).astype(BF16)
        own_ref[i, 0:144] = dot(values, p)
        own_ref[i, 144:152] = jnp.broadcast_to(top, (8, ROWS))
        top = jnp.max(jnp.where(diagonal, dot(oth_keys, q_oth), NEG), axis=0, keepdims=True)
        s = jnp.where(both, dot(keys, q_oth), NEG)
        top = jnp.maximum(top, jnp.max(s, axis=0, keepdims=True))
        p = jnp.exp2(s - top).astype(BF16)
        oth_ref[i, 0:144] = dot(values, p)
        oth_ref[i, 144:152] = jnp.broadcast_to(top, (8, ROWS))
        return carry

    lax.fori_loop(0, MAPS, one_map, 0, unroll=2)


def front_kernel(place_ref, p0, p1a, p1b, p2a, p2b, p3a, p3b, gain_ref, w_ref, normed_ref, kv_ref):
    x = place_ref[3]

    def put(piece_ref, back, half, rows):
        values = piece_ref[...].astype(F32)
        scale = lax.rsqrt(jnp.mean(values * values, axis=1, keepdims=True) + NORM_EPS)
        at = pl.multiple_of(((x - back) & 3) * 64 + half * 32, 32)
        normed_ref[pl.ds(at, rows), :] = (values * scale * gain_ref[...]).astype(BF16)

    put(p0, 0, 0, 64)
    put(p1a, 1, 0, 32)
    put(p1b, 1, 1, 32)
    put(p3a, 3, 0, 32)
    put(p3b, 3, 1, 32)
    put(p2a, 2, 0, 32)
    put(p2b, 2, 1, 32)
    both = dot(normed_ref[...], w_ref[...])
    values_t = both[:, HALF:].T.astype(BF16)
    for half in range(2):
        rows = slice(half * HALF, half * HALF + HALF)
        kv_ref[0, half, :, :HALF] = both[rows, :HALF].astype(BF16)
        kv_ref[0, half, :, HALF:] = values_t[:, rows]


def chunk_kernel(plan, n_in, *refs):
    place_ref, q_ref = refs[0], refs[1]
    ins = refs[2 : 2 + n_in]
    own_in, oth_in, own_ref, oth_ref, keys_ref, values_ref, p_a, p_b, over_ref, list_ref = refs[2 + n_in :]
    probs = (p_a, p_b)
    z, y = place_ref[0], place_ref[1]
    visible = jnp.int32(0)
    at = 0
    for _, offsets in plan:
        for dz, dy in offsets:
            sees = ((z + dz) & 7) * 4 + ((y + dy) & 3) < z * 4 + y
            list_ref[visible] = at
            visible = visible + sees.astype(jnp.int32)
            at += 1

    def fetch(which, slot):
        at = 0
        rows = slice(slot * ROWS, slot * ROWS + HALF), slice(slot * ROWS + HALF, slot * ROWS + ROWS)
        for pair, offsets in plan:
            count = len(offsets)

            @pl.when((which >= at) & (which < at + count))
            def _(pair=pair, at=at):
                b = which - at
                for half in range(2):
                    source = ins[pair].at[b, half]
                    keys_ref[rows[half]] = source[:, :HALF]
                    values_ref[0:HALF, rows[half]] = source[:, HALF:]
            at += count

    own_ref[...] = own_in[...]
    oth_ref[...] = oth_in[...]

    @pl.when(visible > 0)
    def _():
        over_ref[...] = jnp.full(over_ref.shape, NEG, F32)
        values_ref[HALF:144] = jnp.ones((16, 2 * ROWS), BF16)

        def two_blocks(t, carry):
            fetch(list_ref[2 * t], 0)
            second = 2 * t + 1 < visible
            fetch(list_ref[jnp.minimum(2 * t + 1, visible - 1)], 1)

            @pl.when(jnp.logical_not(second))
            def _():
                values_ref[:, ROWS:] = jnp.zeros((144, ROWS), BF16)

            keys, values = keys_ref[...], values_ref[...]

            def scores(i):
                top = jnp.concatenate([own_ref[i, 144:145], oth_ref[i, 144:145]], axis=1)
                s = dot(keys, q_ref[i]) - top
                over_ref[i] = jnp.maximum(over_ref[i], jnp.max(s.reshape(-1, 8, 2 * ROWS), axis=0))
                probs[i % 2][...] = jnp.exp2(s).astype(BF16)

            scores(0)
            for i in range(MAPS):
                if i + 1 < MAPS:
                    scores(i + 1)
                out = dot(values, probs[i % 2][...])
                own_ref[i, 0:144] = own_ref[i, 0:144] + out[:, :ROWS]
                oth_ref[i, 0:144] = oth_ref[i, 0:144] + out[:, ROWS:]
            return carry

        lax.fori_loop(0, (visible + 1) // 2, two_blocks, 0)

        @pl.when(jnp.logical_not(jnp.max(over_ref[...]) <= LIMIT))
        def _():
            own_ref[...] = own_in[...]
            oth_ref[...] = oth_in[...]
            values_ref[HALF:144] = jnp.ones((16, 2 * ROWS), BF16)

            def one_block(t, carry):
                fetch(list_ref[t], 0)

                def one_map(i, carry):
                    before = jnp.concatenate([own_ref[i, 144:145], oth_ref[i, 144:145]], axis=1)
                    s = dot(keys_ref[:ROWS], q_ref[i])
                    top = jnp.maximum(before, jnp.max(s, axis=0, keepdims=True))
                    scale = jnp.exp2(before - top)
                    out = dot(values_ref[:, :ROWS], jnp.exp2(s - top).astype(BF16))
                    top8 = jnp.broadcast_to(top, (8, 2 * ROWS))
                    own_ref[i, 0:144] = own_ref[i, 0:144] * scale[:, :ROWS] + out[:, :ROWS]
                    oth_ref[i, 0:144] = oth_ref[i, 0:144] * scale[:, ROWS:] + out[:, ROWS:]
                    own_ref[i, 144:152] = top8[:, :ROWS]
                    oth_ref[i, 144:152] = top8[:, ROWS:]
                    return carry

                return lax.fori_loop(0, MAPS, one_map, carry)

            lax.fori_loop(0, visible, one_block, 0)


STATE = (pltpu.VMEM((MAPS, ST, ROWS), F32), pltpu.VMEM((MAPS, ST, ROWS), F32))


def in_vmem(array):
    return pltpu.with_memory_space_constraint(array, pltpu.VMEM)


def attend_chunk(place, q, state, plan, arrays, name):
    n = len(arrays)
    blocks = sum(len(offsets) for _, offsets in plan)
    return pl.pallas_call(
        functools.partial(chunk_kernel, plan, n),
        out_shape=STATE,
        in_specs=[SMEM, VMEM] + [VMEM] * n + [VMEM, VMEM],
        out_specs=(VMEM, VMEM),
        scratch_shapes=[
            pltpu.VMEM((2 * ROWS, HALF), BF16),
            pltpu.VMEM((144, 2 * ROWS), BF16),
            pltpu.VMEM((2 * ROWS, 2 * ROWS), BF16),
            pltpu.VMEM((2 * ROWS, 2 * ROWS), BF16),
            pltpu.VMEM((MAPS, 8, 2 * ROWS), F32),
            pltpu.SMEM((blocks + 1,), jnp.int32),
        ],
        cost_estimate=pl.CostEstimate(
            flops=blocks * MAPS * 2 * 256 * 512 * 512, transcendentals=blocks * MAPS * 256 * 512, bytes_accessed=1 << 20
        ),
        compiler_params=vmem(20),
        name=name,
    )(place, in_vmem(q), *arrays, in_vmem(state[0]), in_vmem(state[1]))


def pool_kernel(place_ref, pool_ref, rim_ref, gate_ref, mix_ref, scale_ref, keep_ref, part_ref):
    span = jnp.left_shift(jnp.int32(2), place_ref[3])
    start = ((place_ref[0] * 4 + place_ref[1]) * 2 + place_ref[2]) * ROWS
    now = pool_ref[...].astype(F32)
    sums = jnp.concatenate([rim_ref[...].astype(F32), now], axis=0)
    rows = WINDOW + ROWS
    picked = jnp.zeros((ROWS, now.shape[1]), F32)
    for width in (1, 2, 4, 8):
        sums = sums + jnp.concatenate([jnp.zeros((width, now.shape[1]), F32), sums[: rows - width]], axis=0)
        picked = jnp.where(span == 2 * width, sums[WINDOW:], picked)
    position = start + lax.broadcasted_iota(jnp.int32, (ROWS, 1), 0)
    counts = jnp.minimum(position + 1, span).astype(F32)
    pooled = (picked / counts - now).astype(BF16)
    mixed = dot(pooled, mix_ref[...]) * scale_ref[...]
    width = now.shape[1]
    keep_ref[...] = jax.nn.sigmoid(gate_ref[:, :width].astype(F32))
    part_ref[...] = jax.nn.sigmoid(gate_ref[:, width:].astype(F32)) * mixed


def finish_kernel(lam_ref, a_ref, b_ref, gain_ref, keep_ref, part_ref, w_ref, out_ref, log_ref, merged_ref):
    for h in range(MAPS // 2):
        maps = []
        for m in range(2):
            i = 2 * h + m
            top_a, top_b = a_ref[i, 144:145], b_ref[i, 144:145]
            top = jnp.maximum(top_a, top_b)
            wa, wb = jnp.exp2(top_a - top), jnp.exp2(top_b - top)
            total = a_ref[i, 128:129] * wa + b_ref[i, 128:129] * wb
            log_ref[i : i + 1, :] = (top + jnp.log2(total)) * (1.0 / LOG2E)
            maps.append((a_ref[i, 0:128] * wa + b_ref[i, 0:128] * wb) / total)
        head = maps[0] - lam_ref[h] * maps[1]
        head = head * lax.rsqrt(jnp.mean(head * head, axis=0, keepdims=True) + NORM_EPS)
        cols = slice(h * 128, h * 128 + 128)
        attended = head.T * gain_ref[...]
        merged_ref[:, cols] = (keep_ref[:, cols] * attended + part_ref[:, cols]).astype(BF16)
    out_ref[...] = dot(merged_ref[...], w_ref[...]).astype(BF16)


def local(tokens, norm_gain, query_weight, key_weight, value_weight, mix_lambda, head_gain, pool_weight, pool_mix, pool_scale, gate_weight, out_weight):
    width = tokens.shape[1]
    z, y, c = lax.axis_index("z"), lax.axis_index("y"), lax.axis_index("c")
    place = jnp.stack([z, y, c, lax.axis_index("x")])
    halves = tokens[:32], tokens[32:]
    up_a = lax.ppermute(halves[0], "x", ring(4, 1))
    down_b = lax.ppermute(halves[1], "x", ring(4, -1))
    up_b = lax.ppermute(halves[1], "x", ring(4, 1))
    down_a = lax.ppermute(halves[0], "x", ring(4, -1))
    far_a = lax.ppermute(up_a, "x", ring(4, 1))
    far_b = lax.ppermute(down_b, "x", ring(4, -1))
    gate_w, query_w = gate_weight.reshape(width, -1), query_weight.reshape(width, -1)
    kv_w = jnp.concatenate([key_weight[:, 0], value_weight[:, 0]], axis=1)
    far_a, gate_w, query_w, kv_w = lax.optimization_barrier((far_a, gate_w, query_w, kv_w))
    normed, kv = pl.pallas_call(
        front_kernel,
        out_shape=(jax.ShapeDtypeStruct((ROWS, width), BF16), jax.ShapeDtypeStruct((1, 2, HALF, 2 * HALF), BF16)),
        in_specs=[SMEM] + [VMEM] * 9,
        out_specs=(VMEM, VMEM),
        compiler_params=vmem(16),
        name="front",
    )(place, tokens, up_a, up_b, far_a, far_b, down_a, down_b, norm_gain[None], kv_w)

    def project(weight):
        return dot(normed, weight.reshape(width, -1)).astype(BF16)

    beside = [lax.ppermute(kv, "y", ring(4, step)) for step in (1, -1, 2)]
    group = jnp.concatenate([kv, *beside], axis=0)
    columns = (0, -1, 1, 2)
    up, down = [group], [group]
    for k in range(3):
        up.append(lax.ppermute(up[-1], "z", ring(8, 1)))
        down.append(lax.ppermute(down[-1], "z", ring(8, -1)))
    up.append(lax.ppermute(up[3][:2], "z", ring(8, 1)))
    down.append(lax.ppermute(down[3][2:], "z", ring(8, -1)))

    scale = (query_weight.shape[2] // 2) ** -0.5 * LOG2E
    q_own = (
        lax.dot_general(query_w, normed, (((0,), (1,)), ((), ())), preferred_element_type=F32) * scale
    ).astype(BF16)
    q_oth = lax.ppermute(q_own, "c", [(0, 1), (1, 0)])
    kv_oth = lax.ppermute(kv, "c", [(0, 1), (1, 0)])
    q = jnp.concatenate([q_own, q_oth], axis=1).reshape(4, 2, 64, 2 * ROWS)
    zero = jnp.zeros((4, 64, 2 * ROWS), BF16)
    q = jnp.stack([jnp.concatenate([q[:, 0], zero], axis=1), jnp.concatenate([zero, q[:, 1]], axis=1)], axis=1)
    q = q.reshape(MAPS, 128, 2 * ROWS)

    pool_in = project(pool_weight)
    gate_pre = project(gate_w)
    rim = lax.ppermute(pool_in[ROWS - WINDOW :], ("z", "y", "c"), [(i, i + 1) for i in range(63)])
    part_shape = jax.ShapeDtypeStruct((ROWS, 512), F32)
    keep, part = pl.pallas_call(
        pool_kernel,
        out_shape=(part_shape, part_shape),
        in_specs=[SMEM] + [VMEM] * 5,
        out_specs=(VMEM, VMEM),
        compiler_params=vmem(16),
        name="pool",
    )(place, pool_in, rim, gate_pre, pool_mix[0], pool_scale)

    state = pl.pallas_call(
        first_kernel, out_shape=STATE, in_specs=[SMEM, VMEM, VMEM, VMEM], out_specs=(VMEM, VMEM), compiler_params=vmem(16), name="first"
    )(place, kv, kv_oth, in_vmem(q))
    state, keep, part = lax.optimization_barrier((state, keep, part))
    plan = tuple((i, ((0, dy),)) for i, dy in enumerate(columns[1:]))
    state = attend_chunk(place, q, state, plan, beside, "chunk0")
    for k in range(1, 5):
        plan = (
            (0, tuple((-k, dy) for dy in (columns if k < 4 else columns[:2]))),
            (1, tuple((k, dy) for dy in (columns if k < 4 else columns[2:]))),
        )
        state = attend_chunk(place, q, state, plan, (up[k], down[k]), f"chunk{k}")
    other = lax.ppermute(state[1], "c", [(0, 1), (1, 0)])
    out, logs = pl.pallas_call(
        finish_kernel,
        out_shape=(jax.ShapeDtypeStruct((ROWS, width), BF16), jax.ShapeDtypeStruct((MAPS, ROWS), F32)),
        in_specs=[SMEM] + [VMEM] * 6,
        out_specs=(VMEM, VMEM),
        scratch_shapes=[pltpu.VMEM((ROWS, 512), BF16)],
        compiler_params=vmem(24),
        name="finish",
    )(mix_lambda, state[0], other, head_gain[None], keep, part, out_weight)
    shares = lax.all_to_all(out.reshape(4, 64, width), "x", 0, 0, tiled=True)
    mixed = jnp.sum(shares.astype(F32), axis=0).astype(BF16)
    return mixed, jnp.transpose(logs.reshape(4, 2, ROWS), (1, 0, 2))


def solution(mesh):
    fine = Mesh(mesh.devices.reshape(8, 4, 2, 4), ("z", "y", "c", "x"))
    sp = ("z", "y", "c")
    in_specs = (
        P((*sp, "x"), None),
        P(),
        P(None, "x", None),
        P(None, "x", None),
        P(None, "x", None),
        P("x"),
        P(),
        P(None, "x", None),
        P("x", None, None),
        P("x", None),
        P(None, None, "x"),
        P("x", None),
    )
    out_specs = (P((*sp, "x"), None), P(None, "x", sp))
    return jax.shard_map(local, mesh=fine, in_specs=in_specs, out_specs=out_specs, check_vma=False)
```

```python
import functools
import math

import jax
import jax.numpy as jnp
from jax import lax
from jax.experimental import pallas as pl
from jax.experimental.pallas import tpu as pltpu
from jax.sharding import Mesh
from jax.sharding import PartitionSpec as P

NORM_EPS = 1e-06
WINDOW = 16
ROWS = 256
HALF = 128
MAPS = 8
ST = 152
NEG = -1e30
LIMIT = 64.0
LOG2E = math.log2(math.e)
VMEM = pl.BlockSpec(memory_space=pltpu.VMEM)
SMEM = pl.BlockSpec(memory_space=pltpu.SMEM)
F32 = jnp.float32
BF16 = jnp.bfloat16


def vmem(mib):
    return pltpu.CompilerParams(vmem_limit_bytes=mib << 20)


def ring(size, step):
    return [(i, (i + step) % size) for i in range(size)]


def dot(a, b):
    return jnp.dot(a, b, preferred_element_type=F32)


def with_ones(v0, v1):
    values = jnp.concatenate([v0, v1], axis=1)
    return jnp.concatenate([values, jnp.ones((16, values.shape[1]), BF16)], axis=0)


def first_kernel(place_ref, kv_ref, oth_kv_ref, q_own_ref, q_oth_ref, own_ref, oth_ref, q_ref, p_a, p_b):
    for i in range(MAPS):
        here, there = slice(i % 2 * 64, i % 2 * 64 + 64), slice(64 - i % 2 * 64, 128 - i % 2 * 64)
        q_ref[i, here, :ROWS] = q_own_ref[i * 64 : i * 64 + 64]
        q_ref[i, here, ROWS:] = q_oth_ref[i * 64 : i * 64 + 64]
        q_ref[i, there] = jnp.zeros((64, 2 * ROWS), BF16)
    keys = jnp.concatenate([kv_ref[0, 0, :, :HALF], kv_ref[0, 1, :, :HALF]], axis=0)
    oth_keys = jnp.concatenate([oth_kv_ref[0, 0, :, :HALF], oth_kv_ref[0, 1, :, :HALF]], axis=0)
    values = with_ones(kv_ref[0, 0, :, HALF:], kv_ref[0, 1, :, HALF:])
    row = lax.broadcasted_iota(jnp.int32, (ROWS, 2 * ROWS), 0)
    col = lax.broadcasted_iota(jnp.int32, (ROWS, 2 * ROWS), 1)
    seen = row <= jnp.where(col < ROWS, col, jnp.where(place_ref[2] == 0, ROWS, -1))
    diagonal = (row <= col)[:, :ROWS]
    probs = (p_a, p_b)

    def scores(i, slot):
        s = jnp.where(seen, dot(keys, q_ref[i]), NEG)
        seed = jnp.max(jnp.where(diagonal, dot(oth_keys, q_ref[i, :, ROWS:]), NEG), axis=0, keepdims=True)
        top = jnp.max(s, axis=0, keepdims=True)
        top = jnp.concatenate([top[:, :ROWS], jnp.maximum(top[:, ROWS:], seed)], axis=1)
        probs[slot][...] = jnp.exp2(s - top).astype(BF16)
        own_ref[i, 144:152] = jnp.broadcast_to(top[:, :ROWS], (8, ROWS))
        oth_ref[i, 144:152] = jnp.broadcast_to(top[:, ROWS:], (8, ROWS))

    def sums(i, slot):
        out = dot(values, probs[slot][...])
        own_ref[i, 0:144] = out[:, :ROWS]
        oth_ref[i, 0:144] = out[:, ROWS:]

    def two_maps(h, carry):
        scores(2 * h, 0)
        scores(2 * h + 1, 1)
        sums(2 * h, 0)
        sums(2 * h + 1, 1)
        return carry

    lax.fori_loop(0, MAPS // 2, two_maps, 0)


def join_kernel(a, b, c, d, out_ref):
    for i, ref in enumerate((a, b, c, d)):
        out_ref[i] = ref[0]


def front_kernel(rows_ref, gain_ref, w_ref, normed_ref, kv_ref):
    for j in range(4):
        values = rows_ref[j].astype(F32)
        scale = lax.rsqrt(jnp.mean(values * values, axis=1, keepdims=True) + NORM_EPS)
        normed_ref[j * 64 : j * 64 + 64] = (values * scale * gain_ref[...]).astype(BF16)
    both = dot(normed_ref[...], w_ref[...])
    values_t = both[:, HALF:].T.astype(BF16)
    for half in range(2):
        rows = slice(half * HALF, half * HALF + HALF)
        kv_ref[0, half, :, :HALF] = both[rows, :HALF].astype(BF16)
        kv_ref[0, half, :, HALF:] = values_t[:, rows]


def chunk_kernel(plan, n_in, *refs):
    place_ref, q_ref = refs[0], refs[1]
    ins = refs[2 : 2 + n_in]
    own_in, oth_in, own_ref, oth_ref, keys_ref, values_ref, p_a, p_b, over_ref, list_ref = refs[2 + n_in :]
    probs = (p_a, p_b)
    z, y = place_ref[0], place_ref[1]
    visible = jnp.int32(0)
    at = 0
    for _, offsets in plan:
        for dz, dy in offsets:
            sees = ((z + dz) & 7) * 4 + ((y + dy) & 3) < z * 4 + y
            list_ref[visible] = at
            visible = visible + sees.astype(jnp.int32)
            at += 1

    def fetch(which, slot):
        at = 0
        rows = slice(slot * ROWS, slot * ROWS + HALF), slice(slot * ROWS + HALF, slot * ROWS + ROWS)
        for pair, offsets in plan:
            count = len(offsets)

            @pl.when((which >= at) & (which < at + count))
            def _(pair=pair, at=at):
                b = which - at
                for half in range(2):
                    source = ins[pair].at[b, half]
                    keys_ref[rows[half]] = source[:, :HALF]
                    values_ref[0:HALF, rows[half]] = source[:, HALF:]
            at += count

    own_ref[...] = own_in[...]
    oth_ref[...] = oth_in[...]

    @pl.when(visible > 0)
    def _():
        over_ref[...] = jnp.full(over_ref.shape, NEG, F32)
        values_ref[HALF:144] = jnp.ones((16, 2 * ROWS), BF16)

        def two_blocks(t, carry):
            fetch(list_ref[2 * t], 0)
            second = 2 * t + 1 < visible
            fetch(list_ref[jnp.minimum(2 * t + 1, visible - 1)], 1)

            @pl.when(jnp.logical_not(second))
            def _():
                values_ref[:, ROWS:] = jnp.zeros((144, ROWS), BF16)

            keys, values = keys_ref[...], values_ref[...]

            def scores(i):
                top = jnp.concatenate([own_ref[i, 144:145], oth_ref[i, 144:145]], axis=1)
                s = dot(keys, q_ref[i]) - top
                over_ref[i] = jnp.maximum(over_ref[i], jnp.max(s.reshape(-1, 8, 2 * ROWS), axis=0))
                probs[i % 2][...] = jnp.exp2(s).astype(BF16)

            scores(0)
            for i in range(MAPS):
                if i + 1 < MAPS:
                    scores(i + 1)
                out = dot(values, probs[i % 2][...])
                own_ref[i, 0:144] = own_ref[i, 0:144] + out[:, :ROWS]
                oth_ref[i, 0:144] = oth_ref[i, 0:144] + out[:, ROWS:]
            return carry

        lax.fori_loop(0, (visible + 1) // 2, two_blocks, 0)

        @pl.when(jnp.logical_not(jnp.max(over_ref[...]) <= LIMIT))
        def _():
            own_ref[...] = own_in[...]
            oth_ref[...] = oth_in[...]
            values_ref[HALF:144] = jnp.ones((16, 2 * ROWS), BF16)

            def one_block(t, carry):
                fetch(list_ref[t], 0)

                def one_map(i, carry):
                    before = jnp.concatenate([own_ref[i, 144:145], oth_ref[i, 144:145]], axis=1)
                    s = dot(keys_ref[:ROWS], q_ref[i])
                    top = jnp.maximum(before, jnp.max(s, axis=0, keepdims=True))
                    scale = jnp.exp2(before - top)
                    out = dot(values_ref[:, :ROWS], jnp.exp2(s - top).astype(BF16))
                    top8 = jnp.broadcast_to(top, (8, 2 * ROWS))
                    own_ref[i, 0:144] = own_ref[i, 0:144] * scale[:, :ROWS] + out[:, :ROWS]
                    oth_ref[i, 0:144] = oth_ref[i, 0:144] * scale[:, ROWS:] + out[:, ROWS:]
                    own_ref[i, 144:152] = top8[:, :ROWS]
                    oth_ref[i, 144:152] = top8[:, ROWS:]
                    return carry

                return lax.fori_loop(0, MAPS, one_map, carry)

            lax.fori_loop(0, visible, one_block, 0)


STATE = (pltpu.VMEM((MAPS, ST, ROWS), F32), pltpu.VMEM((MAPS, ST, ROWS), F32))


def in_vmem(array):
    return pltpu.with_memory_space_constraint(array, pltpu.VMEM)


def attend_chunk(place, q, state, plan, arrays, name):
    n = len(arrays)
    blocks = sum(len(offsets) for _, offsets in plan)
    return pl.pallas_call(
        functools.partial(chunk_kernel, plan, n),
        out_shape=STATE,
        in_specs=[SMEM, VMEM] + [VMEM] * n + [VMEM, VMEM],
        out_specs=(VMEM, VMEM),
        scratch_shapes=[
            pltpu.VMEM((2 * ROWS, HALF), BF16),
            pltpu.VMEM((144, 2 * ROWS), BF16),
            pltpu.VMEM((2 * ROWS, 2 * ROWS), BF16),
            pltpu.VMEM((2 * ROWS, 2 * ROWS), BF16),
            pltpu.VMEM((MAPS, 8, 2 * ROWS), F32),
            pltpu.SMEM((blocks + 1,), jnp.int32),
        ],
        cost_estimate=pl.CostEstimate(
            flops=blocks * MAPS * 2 * 256 * 512 * 512, transcendentals=blocks * MAPS * 256 * 512, bytes_accessed=1 << 20
        ),
        compiler_params=vmem(20),
        name=name,
    )(place, in_vmem(q), *arrays, in_vmem(state[0]), in_vmem(state[1]))


def pool_kernel(place_ref, pool_ref, rim_ref, gate_ref, mix_ref, scale_ref, keep_ref, part_ref):
    span = jnp.left_shift(jnp.int32(2), place_ref[3])
    start = ((place_ref[0] * 4 + place_ref[1]) * 2 + place_ref[2]) * ROWS
    now = pool_ref[...].astype(F32)
    sums = jnp.concatenate([rim_ref[...].astype(F32), now], axis=0)
    rows = WINDOW + ROWS
    picked = jnp.zeros((ROWS, now.shape[1]), F32)
    for width in (1, 2, 4, 8):
        sums = sums + jnp.concatenate([jnp.zeros((width, now.shape[1]), F32), sums[: rows - width]], axis=0)
        picked = jnp.where(span == 2 * width, sums[WINDOW:], picked)
    position = start + lax.broadcasted_iota(jnp.int32, (ROWS, 1), 0)
    counts = jnp.minimum(position + 1, span).astype(F32)
    pooled = (picked / counts - now).astype(BF16)
    mixed = dot(pooled, mix_ref[...]) * scale_ref[...]
    width = now.shape[1]
    keep_ref[...] = jax.nn.sigmoid(gate_ref[:, :width].astype(F32))
    part_ref[...] = jax.nn.sigmoid(gate_ref[:, width:].astype(F32)) * mixed


def finish_kernel(place_ref, lam_ref, a_ref, b_ref, gain_ref, keep_ref, part_ref, w_ref, *refs):
    own_out, up_a, up_b, far_a, far_b, down_a, down_b, log_ref, merged_ref = refs
    x = place_ref[3]
    for h in range(MAPS // 2):
        maps = []
        for m in range(2):
            i = 2 * h + m
            top_a, top_b = a_ref[i, 144:145], b_ref[i, 144:145]
            top = jnp.maximum(top_a, top_b)
            wa, wb = jnp.exp2(top_a - top), jnp.exp2(top_b - top)
            total = a_ref[i, 128:129] * wa + b_ref[i, 128:129] * wb
            log_ref[i : i + 1, :] = (top + jnp.log2(total)) * (1.0 / LOG2E)
            maps.append((a_ref[i, 0:128] * wa + b_ref[i, 0:128] * wb) / total)
        head = maps[0] - lam_ref[h] * maps[1]
        head = head * lax.rsqrt(jnp.mean(head * head, axis=0, keepdims=True) + NORM_EPS)
        cols = slice(h * 128, h * 128 + 128)
        merged = (keep_ref[:, cols] * (head.T * gain_ref[...]) + part_ref[:, cols]).astype(BF16)
        for j in range(4):
            at = pl.multiple_of(((j - x) & 3) * 64, 64)
            merged_ref[pl.ds(at, 64), cols] = merged[j * 64 : j * 64 + 64]
    out = dot(merged_ref[...], w_ref[...]).astype(BF16)
    own_out[...] = out[:64]
    for i, ref in enumerate((up_a, up_b, far_a, far_b, down_a, down_b)):
        ref[...] = out[64 + i * 32 : 96 + i * 32]


def local(tokens, norm_gain, query_weight, key_weight, value_weight, mix_lambda, head_gain, pool_weight, pool_mix, pool_scale, gate_weight, out_weight):
    width = tokens.shape[1]
    z, y, c = lax.axis_index("z"), lax.axis_index("y"), lax.axis_index("c")
    place = jnp.stack([z, y, c, lax.axis_index("x")])
    pieces = lax.all_to_all(jnp.broadcast_to(tokens[None], (4, *tokens.shape)), "x", 0, 0, tiled=True)
    gate_w, query_w = gate_weight.reshape(width, -1), query_weight.reshape(width, -1)
    kv_w = jnp.concatenate([key_weight[:, 0], value_weight[:, 0]], axis=1)
    pieces, gate_w, query_w, kv_w = lax.optimization_barrier((pieces, gate_w, query_w, kv_w))
    normed, kv = pl.pallas_call(
        front_kernel,
        out_shape=(jax.ShapeDtypeStruct((ROWS, width), BF16), jax.ShapeDtypeStruct((1, 2, HALF, 2 * HALF), BF16)),
        in_specs=[VMEM] * 3,
        out_specs=(VMEM, VMEM),
        compiler_params=vmem(16),
        name="front",
    )(pieces, norm_gain[None], kv_w)

    def project(weight):
        return dot(normed, weight.reshape(width, -1)).astype(BF16)

    beside = [lax.ppermute(kv, "y", ring(4, step)) for step in (1, -1, 2)]
    group = pl.pallas_call(
        join_kernel,
        out_shape=jax.ShapeDtypeStruct((4, 2, HALF, 2 * HALF), BF16),
        in_specs=[VMEM] * 4,
        out_specs=VMEM,
        compiler_params=vmem(8),
        name="join",
    )(kv, *beside)
    columns = (0, -1, 1, 2)
    up, down = [group], [group]
    for k in range(3):
        up.append(lax.ppermute(up[-1], "z", ring(8, 1)))
        down.append(lax.ppermute(down[-1], "z", ring(8, -1)))
    up.append(lax.ppermute(up[3][:2], "z", ring(8, 1)))
    down.append(lax.ppermute(down[3][2:], "z", ring(8, -1)))

    scale = (query_weight.shape[2] // 2) ** -0.5 * LOG2E
    q_own = (
        lax.dot_general(query_w, normed, (((0,), (1,)), ((), ())), preferred_element_type=F32) * scale
    ).astype(BF16)
    q_oth = lax.ppermute(q_own, "c", [(0, 1), (1, 0)])
    kv_oth = lax.ppermute(kv, "c", [(0, 1), (1, 0)])

    pool_in = project(pool_weight)
    gate_pre = project(gate_w)
    rim = lax.ppermute(pool_in[ROWS - WINDOW :], ("z", "y", "c"), [(i, i + 1) for i in range(63)])
    part_shape = jax.ShapeDtypeStruct((ROWS, 512), F32)
    keep, part = pl.pallas_call(
        pool_kernel,
        out_shape=(part_shape, part_shape),
        in_specs=[SMEM] + [VMEM] * 5,
        out_specs=(VMEM, VMEM),
        compiler_params=vmem(16),
        name="pool",
    )(place, pool_in, rim, gate_pre, pool_mix[0], pool_scale)

    *state, q = pl.pallas_call(
        first_kernel,
        out_shape=(*STATE, pltpu.VMEM((MAPS, 128, 2 * ROWS), BF16)),
        in_specs=[SMEM] + [VMEM] * 4,
        out_specs=(VMEM, VMEM, VMEM),
        scratch_shapes=[pltpu.VMEM((ROWS, 2 * ROWS), BF16)] * 2,
        compiler_params=vmem(16),
        name="first",
    )(place, kv, kv_oth, q_own, q_oth)
    plan = tuple((i, ((0, dy),)) for i, dy in enumerate(columns[1:]))
    state = attend_chunk(place, q, state, plan, beside, "chunk0")
    for k in range(1, 5):
        plan = (
            (0, tuple((-k, dy) for dy in (columns if k < 4 else columns[:2]))),
            (1, tuple((k, dy) for dy in (columns if k < 4 else columns[2:]))),
        )
        state = attend_chunk(place, q, state, plan, (up[k], down[k]), f"chunk{k}")
        if k == 1:
            state, keep, part = lax.optimization_barrier((state, keep, part))
    other = lax.ppermute(state[1], "c", [(0, 1), (1, 0)])
    piece = jax.ShapeDtypeStruct((32, width), BF16)
    own, up_a, up_b, far_a, far_b, down_a, down_b, logs = pl.pallas_call(
        finish_kernel,
        out_shape=(jax.ShapeDtypeStruct((64, width), BF16), *[piece] * 6, jax.ShapeDtypeStruct((MAPS, ROWS), F32)),
        in_specs=[SMEM, SMEM] + [VMEM] * 6,
        out_specs=(VMEM,) * 8,
        scratch_shapes=[pltpu.VMEM((ROWS, 512), BF16)],
        compiler_params=vmem(24),
        name="finish",
    )(place, mix_lambda, state[0], other, head_gain[None], keep, part, out_weight)
    from_far_a = lax.ppermute(far_a, "x", ring(4, 1))
    from_far_b = lax.ppermute(far_b, "x", ring(4, -1))
    low_b = lax.ppermute(up_b, "x", ring(4, 1))
    high_a = lax.ppermute(down_a, "x", ring(4, -1))

    def add(*arrays):
        return sum(a.astype(F32) for a in arrays).astype(BF16)

    low_a = lax.ppermute(add(up_a, from_far_a), "x", ring(4, 1))
    high_b = lax.ppermute(add(down_b, from_far_b), "x", ring(4, -1))
    mixed = jnp.concatenate([add(own[:32], low_a, high_a), add(own[32:], low_b, high_b)], axis=0)
    return mixed, jnp.transpose(logs.reshape(4, 2, ROWS), (1, 0, 2))


def solution(mesh):
    fine = Mesh(mesh.devices.reshape(8, 4, 2, 4), ("z", "y", "c", "x"))
    sp = ("z", "y", "c")
    in_specs = (
        P((*sp, "x"), None),
        P(),
        P(None, "x", None),
        P(None, "x", None),
        P(None, "x", None),
        P("x"),
        P(),
        P(None, "x", None),
        P("x", None, None),
        P("x", None),
        P(None, None, "x"),
        P("x", None),
    )
    out_specs = (P((*sp, "x"), None), P(None, "x", sp))
    return jax.shard_map(local, mesh=fine, in_specs=in_specs, out_specs=out_specs, check_vma=False)
```

```python
import functools
import math

import jax
import jax.numpy as jnp
from jax import lax
from jax.experimental import pallas as pl
from jax.experimental.pallas import tpu as pltpu
from jax.sharding import Mesh
from jax.sharding import PartitionSpec as P

NORM_EPS = 1e-06
WINDOW = 16
ROWS = 256
HALF = 128
MAPS = 8
ST = 152
NEG = -1e30
LIMIT = 64.0
LOG2E = math.log2(math.e)
VMEM = pl.BlockSpec(memory_space=pltpu.VMEM)
SMEM = pl.BlockSpec(memory_space=pltpu.SMEM)
F32 = jnp.float32
BF16 = jnp.bfloat16


def vmem(mib):
    return pltpu.CompilerParams(vmem_limit_bytes=mib << 20)


def ring(size, step):
    return [(i, (i + step) % size) for i in range(size)]


def dot(a, b):
    return jnp.dot(a, b, preferred_element_type=F32)


def with_ones(v0, v1):
    values = jnp.concatenate([v0, v1], axis=1)
    return jnp.concatenate([values, jnp.ones((16, values.shape[1]), BF16)], axis=0)


def first_kernel(place_ref, kv_ref, oth_kv_ref, q_own_ref, q_oth_ref, own_ref, oth_ref, q_ref, p_a, p_b):
    for i in range(MAPS):
        here, there = slice(i % 2 * 64, i % 2 * 64 + 64), slice(64 - i % 2 * 64, 128 - i % 2 * 64)
        q_ref[i, here, :ROWS] = q_own_ref[i * 64 : i * 64 + 64]
        q_ref[i, here, ROWS:] = q_oth_ref[i * 64 : i * 64 + 64]
        q_ref[i, there] = jnp.zeros((64, 2 * ROWS), BF16)
    keys = jnp.concatenate([kv_ref[0, 0, :, :HALF], kv_ref[0, 1, :, :HALF]], axis=0)
    oth_keys = jnp.concatenate([oth_kv_ref[0, 0, :, :HALF], oth_kv_ref[0, 1, :, :HALF]], axis=0)
    values = with_ones(kv_ref[0, 0, :, HALF:], kv_ref[0, 1, :, HALF:])
    row = lax.broadcasted_iota(jnp.int32, (ROWS, 2 * ROWS), 0)
    col = lax.broadcasted_iota(jnp.int32, (ROWS, 2 * ROWS), 1)
    seen = row <= jnp.where(col < ROWS, col, jnp.where(place_ref[2] == 0, ROWS, -1))
    diagonal = (row <= col)[:, :ROWS]
    probs = (p_a, p_b)

    def scores(i, slot):
        s = jnp.where(seen, dot(keys, q_ref[i]), NEG)
        seed = jnp.max(jnp.where(diagonal, dot(oth_keys, q_ref[i, :, ROWS:]), NEG), axis=0, keepdims=True)
        top = jnp.max(s, axis=0, keepdims=True)
        top = jnp.concatenate([top[:, :ROWS], jnp.maximum(top[:, ROWS:], seed)], axis=1)
        probs[slot][...] = jnp.exp2(s - top).astype(BF16)
        own_ref[i, 144:152] = jnp.broadcast_to(top[:, :ROWS], (8, ROWS))
        oth_ref[i, 144:152] = jnp.broadcast_to(top[:, ROWS:], (8, ROWS))

    def sums(i, slot):
        out = dot(values, probs[slot][...])
        own_ref[i, 0:144] = out[:, :ROWS]
        oth_ref[i, 0:144] = out[:, ROWS:]

    def two_maps(h, carry):
        scores(2 * h, 0)
        scores(2 * h + 1, 1)
        sums(2 * h, 0)
        sums(2 * h + 1, 1)
        return carry

    lax.fori_loop(0, MAPS // 2, two_maps, 0)


def join_kernel(a, b, c, d, out_ref):
    for i, ref in enumerate((a, b, c, d)):
        out_ref[i] = ref[0]


def front_kernel(rows_ref, gain_ref, w_ref, normed_ref, kv_ref):
    for j in range(4):
        values = rows_ref[j].astype(F32)
        scale = lax.rsqrt(jnp.mean(values * values, axis=1, keepdims=True) + NORM_EPS)
        normed_ref[j * 64 : j * 64 + 64] = (values * scale * gain_ref[...]).astype(BF16)
    both = dot(normed_ref[...], w_ref[...])
    values_t = both[:, HALF:].T.astype(BF16)
    for half in range(2):
        rows = slice(half * HALF, half * HALF + HALF)
        kv_ref[0, half, :, :HALF] = both[rows, :HALF].astype(BF16)
        kv_ref[0, half, :, HALF:] = values_t[:, rows]


def chunk_kernel(plan, n_in, *refs):
    place_ref, q_ref = refs[0], refs[1]
    ins = refs[2 : 2 + n_in]
    own_in, oth_in, own_ref, oth_ref, keys_ref, values_ref, p_a, p_b, over_ref, list_ref = refs[2 + n_in :]
    probs = (p_a, p_b)
    z, y = place_ref[0], place_ref[1]
    visible = jnp.int32(0)
    at = 0
    for _, offsets in plan:
        for dz, dy in offsets:
            sees = ((z + dz) & 7) * 4 + ((y + dy) & 3) < z * 4 + y
            list_ref[visible] = at
            visible = visible + sees.astype(jnp.int32)
            at += 1

    def fetch(which, slot):
        at = 0
        rows = slice(slot * ROWS, slot * ROWS + HALF), slice(slot * ROWS + HALF, slot * ROWS + ROWS)
        for pair, offsets in plan:
            count = len(offsets)

            @pl.when((which >= at) & (which < at + count))
            def _(pair=pair, at=at):
                b = which - at
                for half in range(2):
                    source = ins[pair].at[b, half]
                    keys_ref[rows[half]] = source[:, :HALF]
                    values_ref[0:HALF, rows[half]] = source[:, HALF:]
            at += count

    def keep_state():
        own_ref[...] = own_in[...]
        oth_ref[...] = oth_in[...]

    pl.when(visible == 0)(keep_state)

    @pl.when(visible > 0)
    def _():
        own_ref[:, 144:] = own_in[:, 144:]
        oth_ref[:, 144:] = oth_in[:, 144:]
        over_ref[...] = jnp.full(over_ref.shape, NEG, F32)
        values_ref[HALF:144] = jnp.ones((16, 2 * ROWS), BF16)

        def two_blocks(t, carry):
            fetch(list_ref[2 * t], 0)
            second = 2 * t + 1 < visible
            fetch(list_ref[jnp.minimum(2 * t + 1, visible - 1)], 1)

            @pl.when(jnp.logical_not(second))
            def _():
                values_ref[:, ROWS:] = jnp.zeros((144, ROWS), BF16)

            keys, values = keys_ref[...], values_ref[...]

            def scores(i):
                top = jnp.concatenate([own_in[i, 144:145], oth_in[i, 144:145]], axis=1)
                s = dot(keys, q_ref[i]) - top
                over_ref[i] = jnp.maximum(over_ref[i], jnp.max(s.reshape(-1, 8, 2 * ROWS), axis=0))
                probs[i % 2][...] = jnp.exp2(s).astype(BF16)

            scores(0)
            for i in range(MAPS):
                if i + 1 < MAPS:
                    scores(i + 1)
                out = dot(values, probs[i % 2][...])
                own_ref[i, 0:144] = jnp.where(t == 0, own_in[i, 0:144], own_ref[i, 0:144]) + out[:, :ROWS]
                oth_ref[i, 0:144] = jnp.where(t == 0, oth_in[i, 0:144], oth_ref[i, 0:144]) + out[:, ROWS:]
            return carry

        lax.fori_loop(0, (visible + 1) // 2, two_blocks, 0)

        @pl.when(jnp.logical_not(jnp.max(over_ref[...]) <= LIMIT))
        def _():
            keep_state()
            values_ref[HALF:144] = jnp.ones((16, 2 * ROWS), BF16)

            def one_block(t, carry):
                fetch(list_ref[t], 0)

                def one_map(i, carry):
                    before = jnp.concatenate([own_ref[i, 144:145], oth_ref[i, 144:145]], axis=1)
                    s = dot(keys_ref[:ROWS], q_ref[i])
                    top = jnp.maximum(before, jnp.max(s, axis=0, keepdims=True))
                    scale = jnp.exp2(before - top)
                    out = dot(values_ref[:, :ROWS], jnp.exp2(s - top).astype(BF16))
                    top8 = jnp.broadcast_to(top, (8, 2 * ROWS))
                    own_ref[i, 0:144] = own_ref[i, 0:144] * scale[:, :ROWS] + out[:, :ROWS]
                    oth_ref[i, 0:144] = oth_ref[i, 0:144] * scale[:, ROWS:] + out[:, ROWS:]
                    own_ref[i, 144:152] = top8[:, :ROWS]
                    oth_ref[i, 144:152] = top8[:, ROWS:]
                    return carry

                return lax.fori_loop(0, MAPS, one_map, carry)

            lax.fori_loop(0, visible, one_block, 0)


STATE = (pltpu.VMEM((MAPS, ST, ROWS), F32), pltpu.VMEM((MAPS, ST, ROWS), F32))


def in_vmem(array):
    return pltpu.with_memory_space_constraint(array, pltpu.VMEM)


def attend_chunk(place, q, state, plan, arrays, name):
    n = len(arrays)
    blocks = sum(len(offsets) for _, offsets in plan)
    return pl.pallas_call(
        functools.partial(chunk_kernel, plan, n),
        out_shape=STATE,
        in_specs=[SMEM, VMEM] + [VMEM] * n + [VMEM, VMEM],
        out_specs=(VMEM, VMEM),
        scratch_shapes=[
            pltpu.VMEM((2 * ROWS, HALF), BF16),
            pltpu.VMEM((144, 2 * ROWS), BF16),
            pltpu.VMEM((2 * ROWS, 2 * ROWS), BF16),
            pltpu.VMEM((2 * ROWS, 2 * ROWS), BF16),
            pltpu.VMEM((MAPS, 8, 2 * ROWS), F32),
            pltpu.SMEM((blocks + 1,), jnp.int32),
        ],
        cost_estimate=pl.CostEstimate(
            flops=blocks * MAPS * 2 * 256 * 512 * 512, transcendentals=blocks * MAPS * 256 * 512, bytes_accessed=1 << 20
        ),
        compiler_params=vmem(20),
        name=name,
    )(place, in_vmem(q), *arrays, in_vmem(state[0]), in_vmem(state[1]))


def pool_kernel(place_ref, pool_ref, rim_ref, gate_ref, mix_ref, scale_ref, keep_ref, part_ref):
    span = jnp.left_shift(jnp.int32(2), place_ref[3])
    start = ((place_ref[0] * 4 + place_ref[1]) * 2 + place_ref[2]) * ROWS
    now = pool_ref[...].astype(F32)
    sums = jnp.concatenate([rim_ref[...].astype(F32), now], axis=0)
    rows = WINDOW + ROWS
    picked = jnp.zeros((ROWS, now.shape[1]), F32)
    for width in (1, 2, 4, 8):
        sums = sums + jnp.concatenate([jnp.zeros((width, now.shape[1]), F32), sums[: rows - width]], axis=0)
        picked = jnp.where(span == 2 * width, sums[WINDOW:], picked)
    position = start + lax.broadcasted_iota(jnp.int32, (ROWS, 1), 0)
    counts = jnp.minimum(position + 1, span).astype(F32)
    pooled = (picked / counts - now).astype(BF16)
    mixed = dot(pooled, mix_ref[...]) * scale_ref[...]
    width = now.shape[1]
    keep_ref[...] = jax.nn.sigmoid(gate_ref[:, :width].astype(F32))
    part_ref[...] = jax.nn.sigmoid(gate_ref[:, width:].astype(F32)) * mixed


def finish_kernel(place_ref, lam_ref, a_ref, b_ref, gain_ref, keep_ref, part_ref, w_ref, *refs):
    own_out, up_a, up_b, far_a, far_b, down_a, down_b, log_ref, merged_ref = refs
    x = place_ref[3]
    for h in range(MAPS // 2):
        maps = []
        for m in range(2):
            i = 2 * h + m
            top_a, top_b = a_ref[i, 144:145], b_ref[i, 144:145]
            top = jnp.maximum(top_a, top_b)
            wa, wb = jnp.exp2(top_a - top), jnp.exp2(top_b - top)
            total = a_ref[i, 128:129] * wa + b_ref[i, 128:129] * wb
            log_ref[i : i + 1, :] = (top + jnp.log2(total)) * (1.0 / LOG2E)
            maps.append((a_ref[i, 0:128] * wa + b_ref[i, 0:128] * wb) / total)
        head = maps[0] - lam_ref[h] * maps[1]
        head = head * lax.rsqrt(jnp.mean(head * head, axis=0, keepdims=True) + NORM_EPS)
        cols = slice(h * 128, h * 128 + 128)
        merged = (keep_ref[:, cols] * (head.T * gain_ref[...]) + part_ref[:, cols]).astype(BF16)
        for j in range(4):
            at = pl.multiple_of(((j - x) & 3) * 64, 64)
            merged_ref[pl.ds(at, 64), cols] = merged[j * 64 : j * 64 + 64]
    out = dot(merged_ref[...], w_ref[...]).astype(BF16)
    own_out[...] = out[:64]
    for i, ref in enumerate((up_a, up_b, far_a, far_b, down_a, down_b)):
        ref[...] = out[64 + i * 32 : 96 + i * 32]


def local(tokens, norm_gain, query_weight, key_weight, value_weight, mix_lambda, head_gain, pool_weight, pool_mix, pool_scale, gate_weight, out_weight):
    width = tokens.shape[1]
    z, y, c = lax.axis_index("z"), lax.axis_index("y"), lax.axis_index("c")
    place = jnp.stack([z, y, c, lax.axis_index("x")])
    pieces = lax.all_to_all(jnp.broadcast_to(tokens[None], (4, *tokens.shape)), "x", 0, 0, tiled=True)
    gate_w, query_w = gate_weight.reshape(width, -1), query_weight.reshape(width, -1)
    kv_w = jnp.concatenate([key_weight[:, 0], value_weight[:, 0]], axis=1)
    pieces, gate_w, query_w, kv_w = lax.optimization_barrier((pieces, gate_w, query_w, kv_w))
    normed, kv = pl.pallas_call(
        front_kernel,
        out_shape=(jax.ShapeDtypeStruct((ROWS, width), BF16), jax.ShapeDtypeStruct((1, 2, HALF, 2 * HALF), BF16)),
        in_specs=[VMEM] * 3,
        out_specs=(VMEM, VMEM),
        compiler_params=vmem(16),
        name="front",
    )(pieces, norm_gain[None], kv_w)

    beside = [lax.ppermute(kv, "y", ring(4, step)) for step in (1, -1, 2)]
    group = pl.pallas_call(
        join_kernel,
        out_shape=jax.ShapeDtypeStruct((4, 2, HALF, 2 * HALF), BF16),
        in_specs=[VMEM] * 4,
        out_specs=VMEM,
        compiler_params=vmem(8),
        name="join",
    )(kv, *beside)
    columns = (0, -1, 1, 2)
    up, down = [group], [group]
    for k in range(3):
        up.append(lax.ppermute(up[-1], "z", ring(8, 1)))
        down.append(lax.ppermute(down[-1], "z", ring(8, -1)))
    up.append(lax.ppermute(up[3][:2], "z", ring(8, 1)))
    down.append(lax.ppermute(down[3][2:], "z", ring(8, -1)))

    scale = (query_weight.shape[2] // 2) ** -0.5 * LOG2E
    q_own = (
        lax.dot_general(query_w, normed, (((0,), (1,)), ((), ())), preferred_element_type=F32) * scale
    ).astype(BF16)
    q_oth = lax.ppermute(q_own, "c", [(0, 1), (1, 0)])
    kv_oth = lax.ppermute(kv, "c", [(0, 1), (1, 0)])

    *state, q = pl.pallas_call(
        first_kernel,
        out_shape=(*STATE, pltpu.VMEM((MAPS, 128, 2 * ROWS), BF16)),
        in_specs=[SMEM] + [VMEM] * 4,
        out_specs=(VMEM, VMEM, VMEM),
        scratch_shapes=[pltpu.VMEM((ROWS, 2 * ROWS), BF16)] * 2,
        compiler_params=vmem(16),
        name="first",
    )(place, kv, kv_oth, q_own, q_oth)
    plan = tuple((i, ((0, dy),)) for i, dy in enumerate(columns[1:]))
    state = attend_chunk(place, q, state, plan, beside, "chunk0")
    normed, state = lax.optimization_barrier((normed, state))
    pool_in = dot(normed, pool_weight[:, 0]).astype(BF16)
    rim = lax.ppermute(pool_in[ROWS - WINDOW :], ("z", "y", "c"), [(i, i + 1) for i in range(63)])
    for k in range(1, 5):
        plan = (
            (0, tuple((-k, dy) for dy in (columns if k < 4 else columns[:2]))),
            (1, tuple((k, dy) for dy in (columns if k < 4 else columns[2:]))),
        )
        state = attend_chunk(place, q, state, plan, (up[k], down[k]), f"chunk{k}")
        if k == 1:
            normed, state = lax.optimization_barrier((normed, state))
            gate_pre = dot(normed, gate_w).astype(BF16)
        if k == 2:
            gate_pre, state = lax.optimization_barrier((gate_pre, state))
            part_shape = jax.ShapeDtypeStruct((ROWS, 512), F32)
            keep, part = pl.pallas_call(
                pool_kernel,
                out_shape=(part_shape, part_shape),
                in_specs=[SMEM] + [VMEM] * 5,
                out_specs=(VMEM, VMEM),
                compiler_params=vmem(16),
                name="pool",
            )(place, pool_in, rim, gate_pre, pool_mix[0], pool_scale)
            state, keep, part = lax.optimization_barrier((state, keep, part))
    other = lax.ppermute(state[1], "c", [(0, 1), (1, 0)])
    piece = jax.ShapeDtypeStruct((32, width), BF16)
    own, up_a, up_b, far_a, far_b, down_a, down_b, logs = pl.pallas_call(
        finish_kernel,
        out_shape=(jax.ShapeDtypeStruct((64, width), BF16), *[piece] * 6, jax.ShapeDtypeStruct((MAPS, ROWS), F32)),
        in_specs=[SMEM, SMEM] + [VMEM] * 6,
        out_specs=(VMEM,) * 8,
        scratch_shapes=[pltpu.VMEM((ROWS, 512), BF16)],
        compiler_params=vmem(24),
        name="finish",
    )(place, mix_lambda, state[0], other, head_gain[None], keep, part, out_weight)
    from_far_a = lax.ppermute(far_a, "x", ring(4, 1))
    from_far_b = lax.ppermute(far_b, "x", ring(4, -1))
    low_b = lax.ppermute(up_b, "x", ring(4, 1))
    high_a = lax.ppermute(down_a, "x", ring(4, -1))

    def add(*arrays):
        return sum(a.astype(F32) for a in arrays).astype(BF16)

    low_a = lax.ppermute(add(up_a, from_far_a), "x", ring(4, 1))
    high_b = lax.ppermute(add(down_b, from_far_b), "x", ring(4, -1))
    mixed = jnp.concatenate([add(own[:32], low_a, high_a), add(own[32:], low_b, high_b)], axis=0)
    return mixed, jnp.transpose(logs.reshape(4, 2, ROWS), (1, 0, 2))


def solution(mesh):
    fine = Mesh(mesh.devices.reshape(8, 4, 2, 4), ("z", "y", "c", "x"))
    sp = ("z", "y", "c")
    in_specs = (
        P((*sp, "x"), None),
        P(),
        P(None, "x", None),
        P(None, "x", None),
        P(None, "x", None),
        P("x"),
        P(),
        P(None, "x", None),
        P("x", None, None),
        P("x", None),
        P(None, None, "x"),
        P("x", None),
    )
    out_specs = (P((*sp, "x"), None), P(None, "x", sp))
    return jax.shard_map(local, mesh=fine, in_specs=in_specs, out_specs=out_specs, check_vma=False)
```

```python
import functools
import math

import jax
import jax.numpy as jnp
from jax import lax
from jax.experimental import pallas as pl
from jax.experimental.pallas import tpu as pltpu
from jax.sharding import Mesh
from jax.sharding import PartitionSpec as P

NORM_EPS = 1e-06
WINDOW = 16
ROWS = 256
HALF = 128
MAPS = 8
ST = 152
NEG = -1e30
LIMIT = 64.0
LOG2E = math.log2(math.e)
VMEM = pl.BlockSpec(memory_space=pltpu.VMEM)
SMEM = pl.BlockSpec(memory_space=pltpu.SMEM)
F32 = jnp.float32
BF16 = jnp.bfloat16


def vmem(mib):
    return pltpu.CompilerParams(vmem_limit_bytes=mib << 20)


def ring(size, step):
    return [(i, (i + step) % size) for i in range(size)]


def dot(a, b):
    return jnp.dot(a, b, preferred_element_type=F32)


def with_ones(v0, v1):
    values = jnp.concatenate([v0, v1], axis=1)
    return jnp.concatenate([values, jnp.ones((16, values.shape[1]), BF16)], axis=0)


def first_kernel(place_ref, kv_ref, oth_kv_ref, q_own_ref, q_oth_ref, own_ref, oth_ref, q_ref, p_a, p_b):
    for i in range(MAPS):
        here, there = slice(i % 2 * 64, i % 2 * 64 + 64), slice(64 - i % 2 * 64, 128 - i % 2 * 64)
        q_ref[i, here, :ROWS] = q_own_ref[i * 64 : i * 64 + 64]
        q_ref[i, here, ROWS:] = q_oth_ref[i * 64 : i * 64 + 64]
        q_ref[i, there] = jnp.zeros((64, 2 * ROWS), BF16)
    keys = jnp.concatenate([kv_ref[0, 0, :, :HALF], kv_ref[0, 1, :, :HALF]], axis=0)
    oth_keys = jnp.concatenate([oth_kv_ref[0, 0, :, :HALF], oth_kv_ref[0, 1, :, :HALF]], axis=0)
    values = with_ones(kv_ref[0, 0, :, HALF:], kv_ref[0, 1, :, HALF:])
    row = lax.broadcasted_iota(jnp.int32, (ROWS, 2 * ROWS), 0)
    col = lax.broadcasted_iota(jnp.int32, (ROWS, 2 * ROWS), 1)
    seen = row <= jnp.where(col < ROWS, col, jnp.where(place_ref[2] == 0, ROWS, -1))
    diagonal = (row <= col)[:, :ROWS]
    probs = (p_a, p_b)

    def scores(i, slot):
        s = jnp.where(seen, dot(keys, q_ref[i]), NEG)
        seed = jnp.max(jnp.where(diagonal, dot(oth_keys, q_ref[i, :, ROWS:]), NEG), axis=0, keepdims=True)
        top = jnp.max(s, axis=0, keepdims=True)
        top = jnp.concatenate([top[:, :ROWS], jnp.maximum(top[:, ROWS:], seed)], axis=1)
        probs[slot][...] = jnp.exp2(s - top).astype(BF16)
        own_ref[i, 144:152] = jnp.broadcast_to(top[:, :ROWS], (8, ROWS))
        oth_ref[i, 144:152] = jnp.broadcast_to(top[:, ROWS:], (8, ROWS))

    def sums(i, slot):
        out = dot(values, probs[slot][...])
        own_ref[i, 0:144] = out[:, :ROWS]
        oth_ref[i, 0:144] = out[:, ROWS:]

    def two_maps(h, carry):
        scores(2 * h, 0)
        scores(2 * h + 1, 1)
        sums(2 * h, 0)
        sums(2 * h + 1, 1)
        return carry

    lax.fori_loop(0, MAPS // 2, two_maps, 0)


def join_kernel(a, b, c, d, out_ref):
    for i, ref in enumerate((a, b, c, d)):
        out_ref[i] = ref[0]


def front_kernel(place_ref, p0, p1a, p1b, p2a, p2b, p3a, p3b, gain_ref, w_ref, normed_ref, kv_ref):
    x = place_ref[3]

    def put(piece_ref, back, half, rows):
        values = piece_ref[...].astype(F32)
        scale = lax.rsqrt(jnp.mean(values * values, axis=1, keepdims=True) + NORM_EPS)
        at = pl.multiple_of(((x - back) & 3) * 64 + half * 32, 32)
        normed_ref[pl.ds(at, rows), :] = (values * scale * gain_ref[...]).astype(BF16)

    put(p0, 0, 0, 64)
    put(p1a, 1, 0, 32)
    put(p1b, 1, 1, 32)
    put(p3a, 3, 0, 32)
    put(p3b, 3, 1, 32)
    put(p2a, 2, 0, 32)
    put(p2b, 2, 1, 32)
    both = dot(normed_ref[...], w_ref[...])
    values_t = both[:, HALF:].T.astype(BF16)
    for half in range(2):
        rows = slice(half * HALF, half * HALF + HALF)
        kv_ref[0, half, :, :HALF] = both[rows, :HALF].astype(BF16)
        kv_ref[0, half, :, HALF:] = values_t[:, rows]


def chunk_kernel(plan, n_in, rolled, *refs):
    place_ref, q_ref = refs[0], refs[1]
    ins = refs[2 : 2 + n_in]
    own_in, oth_in, own_ref, oth_ref, keys_ref, values_ref, p_a, p_b, over_ref, list_ref = refs[2 + n_in :]
    probs = (p_a, p_b)
    z, y = place_ref[0], place_ref[1]
    visible = jnp.int32(0)
    at = 0
    for _, offsets in plan:
        for dz, dy in offsets:
            sees = ((z + dz) & 7) * 4 + ((y + dy) & 3) < z * 4 + y
            list_ref[visible] = at
            visible = visible + sees.astype(jnp.int32)
            at += 1

    def fetch(which, slot):
        at = 0
        rows = slice(slot * ROWS, slot * ROWS + HALF), slice(slot * ROWS + HALF, slot * ROWS + ROWS)
        for pair, offsets in plan:
            count = len(offsets)

            @pl.when((which >= at) & (which < at + count))
            def _(pair=pair, at=at):
                b = which - at
                for half in range(2):
                    source = ins[pair].at[b, half]
                    keys_ref[rows[half]] = source[:, :HALF]
                    values_ref[0:HALF, rows[half]] = source[:, HALF:]
            at += count

    def keep_state():
        own_ref[...] = own_in[...]
        oth_ref[...] = oth_in[...]

    pl.when(visible == 0)(keep_state)

    @pl.when(visible > 0)
    def _():
        own_ref[:, 144:] = own_in[:, 144:]
        oth_ref[:, 144:] = oth_in[:, 144:]
        over_ref[...] = jnp.full(over_ref.shape, NEG, F32)
        values_ref[HALF:144] = jnp.ones((16, 2 * ROWS), BF16)

        def two_blocks(t, carry):
            fetch(list_ref[2 * t], 0)
            second = 2 * t + 1 < visible
            fetch(list_ref[jnp.minimum(2 * t + 1, visible - 1)], 1)

            @pl.when(jnp.logical_not(second))
            def _():
                values_ref[:, ROWS:] = jnp.zeros((144, ROWS), BF16)

            keys, values = keys_ref[...], values_ref[...]

            def scores(i, slot):
                top = jnp.concatenate([own_in[i, 144:145], oth_in[i, 144:145]], axis=1)
                s = dot(keys, q_ref[i]) - top
                over_ref[i] = jnp.maximum(over_ref[i], jnp.max(s.reshape(-1, 8, 2 * ROWS), axis=0))
                probs[slot][...] = jnp.exp2(s).astype(BF16)

            def sums(i, slot):
                out = dot(values, probs[slot][...])
                own_ref[i, 0:144] = jnp.where(t == 0, own_in[i, 0:144], own_ref[i, 0:144]) + out[:, :ROWS]
                oth_ref[i, 0:144] = jnp.where(t == 0, oth_in[i, 0:144], oth_ref[i, 0:144]) + out[:, ROWS:]

            def two_maps(h, carry):
                scores(2 * h, 0)
                scores(2 * h + 1, 1)
                sums(2 * h, 0)
                sums(2 * h + 1, 1)
                return carry

            if rolled:
                return lax.fori_loop(0, MAPS // 2, two_maps, carry)
            scores(0, 0)
            for i in range(MAPS):
                if i + 1 < MAPS:
                    scores(i + 1, (i + 1) % 2)
                sums(i, i % 2)
            return carry

        lax.fori_loop(0, (visible + 1) // 2, two_blocks, 0)

        @pl.when(jnp.logical_not(jnp.max(over_ref[...]) <= LIMIT))
        def _():
            keep_state()
            values_ref[HALF:144] = jnp.ones((16, 2 * ROWS), BF16)

            def one_block(t, carry):
                fetch(list_ref[t], 0)

                def one_map(i, carry):
                    before = jnp.concatenate([own_ref[i, 144:145], oth_ref[i, 144:145]], axis=1)
                    s = dot(keys_ref[:ROWS], q_ref[i])
                    top = jnp.maximum(before, jnp.max(s, axis=0, keepdims=True))
                    scale = jnp.exp2(before - top)
                    out = dot(values_ref[:, :ROWS], jnp.exp2(s - top).astype(BF16))
                    top8 = jnp.broadcast_to(top, (8, 2 * ROWS))
                    own_ref[i, 0:144] = own_ref[i, 0:144] * scale[:, :ROWS] + out[:, :ROWS]
                    oth_ref[i, 0:144] = oth_ref[i, 0:144] * scale[:, ROWS:] + out[:, ROWS:]
                    own_ref[i, 144:152] = top8[:, :ROWS]
                    oth_ref[i, 144:152] = top8[:, ROWS:]
                    return carry

                return lax.fori_loop(0, MAPS, one_map, carry)

            lax.fori_loop(0, visible, one_block, 0)


STATE = (pltpu.VMEM((MAPS, ST, ROWS), F32), pltpu.VMEM((MAPS, ST, ROWS), F32))


def in_vmem(array):
    return pltpu.with_memory_space_constraint(array, pltpu.VMEM)


def attend_chunk(place, q, state, plan, arrays, name, rolled=False):
    n = len(arrays)
    blocks = sum(len(offsets) for _, offsets in plan)
    return pl.pallas_call(
        functools.partial(chunk_kernel, plan, n, rolled),
        out_shape=STATE,
        in_specs=[SMEM, VMEM] + [VMEM] * n + [VMEM, VMEM],
        out_specs=(VMEM, VMEM),
        scratch_shapes=[
            pltpu.VMEM((2 * ROWS, HALF), BF16),
            pltpu.VMEM((144, 2 * ROWS), BF16),
            pltpu.VMEM((2 * ROWS, 2 * ROWS), BF16),
            pltpu.VMEM((2 * ROWS, 2 * ROWS), BF16),
            pltpu.VMEM((MAPS, 8, 2 * ROWS), F32),
            pltpu.SMEM((blocks + 1,), jnp.int32),
        ],
        cost_estimate=pl.CostEstimate(
            flops=blocks * MAPS * 2 * 256 * 512 * 512, transcendentals=blocks * MAPS * 256 * 512, bytes_accessed=1 << 20
        ),
        compiler_params=vmem(20),
        name=name,
    )(place, in_vmem(q), *arrays, in_vmem(state[0]), in_vmem(state[1]))


def pool_kernel(place_ref, pool_ref, rim_ref, gate_ref, mix_ref, scale_ref, keep_ref, part_ref):
    span = jnp.left_shift(jnp.int32(2), place_ref[3])
    start = ((place_ref[0] * 4 + place_ref[1]) * 2 + place_ref[2]) * ROWS
    now = pool_ref[...].astype(F32)
    sums = jnp.concatenate([rim_ref[...].astype(F32), now], axis=0)
    rows = WINDOW + ROWS
    picked = jnp.zeros((ROWS, now.shape[1]), F32)
    for width in (1, 2, 4, 8):
        sums = sums + jnp.concatenate([jnp.zeros((width, now.shape[1]), F32), sums[: rows - width]], axis=0)
        picked = jnp.where(span == 2 * width, sums[WINDOW:], picked)
    position = start + lax.broadcasted_iota(jnp.int32, (ROWS, 1), 0)
    counts = jnp.minimum(position + 1, span).astype(F32)
    pooled = (picked / counts - now).astype(BF16)
    mixed = dot(pooled, mix_ref[...]) * scale_ref[...]
    width = now.shape[1]
    keep_ref[...] = jax.nn.sigmoid(gate_ref[:, :width].astype(F32))
    part_ref[...] = jax.nn.sigmoid(gate_ref[:, width:].astype(F32)) * mixed


def finish_kernel(place_ref, lam_ref, a_ref, b_ref, gain_ref, keep_ref, part_ref, w_ref, *refs):
    own_out, up_a, up_b, far_a, far_b, down_a, down_b, log_ref, merged_ref = refs
    x = place_ref[3]
    for h in range(MAPS // 2):
        maps = []
        for m in range(2):
            i = 2 * h + m
            top_a, top_b = a_ref[i, 144:145], b_ref[i, 144:145]
            top = jnp.maximum(top_a, top_b)
            wa, wb = jnp.exp2(top_a - top), jnp.exp2(top_b - top)
            total = a_ref[i, 128:129] * wa + b_ref[i, 128:129] * wb
            log_ref[i : i + 1, :] = (top + jnp.log2(total)) * (1.0 / LOG2E)
            maps.append((a_ref[i, 0:128] * wa + b_ref[i, 0:128] * wb) / total)
        head = maps[0] - lam_ref[h] * maps[1]
        head = head * lax.rsqrt(jnp.mean(head * head, axis=0, keepdims=True) + NORM_EPS)
        cols = slice(h * 128, h * 128 + 128)
        merged = (keep_ref[:, cols] * (head.T * gain_ref[...]) + part_ref[:, cols]).astype(BF16)
        for j in range(4):
            at = pl.multiple_of(((j - x) & 3) * 64, 64)
            merged_ref[pl.ds(at, 64), cols] = merged[j * 64 : j * 64 + 64]
    out = dot(merged_ref[...], w_ref[...]).astype(BF16)
    own_out[...] = out[:64]
    for i, ref in enumerate((up_a, up_b, far_a, far_b, down_a, down_b)):
        ref[...] = out[64 + i * 32 : 96 + i * 32]


def local(tokens, norm_gain, query_weight, key_weight, value_weight, mix_lambda, head_gain, pool_weight, pool_mix, pool_scale, gate_weight, out_weight):
    width = tokens.shape[1]
    z, y, c = lax.axis_index("z"), lax.axis_index("y"), lax.axis_index("c")
    place = jnp.stack([z, y, c, lax.axis_index("x")])
    halves = tokens[:32], tokens[32:]
    up_a = lax.ppermute(halves[0], "x", ring(4, 1))
    down_b = lax.ppermute(halves[1], "x", ring(4, -1))
    up_b = lax.ppermute(halves[1], "x", ring(4, 1))
    down_a = lax.ppermute(halves[0], "x", ring(4, -1))
    far_a = lax.ppermute(up_a, "x", ring(4, 1))
    far_b = lax.ppermute(down_b, "x", ring(4, -1))
    kv_w = jnp.concatenate([key_weight[:, 0], value_weight[:, 0]], axis=1)
    normed, kv = pl.pallas_call(
        front_kernel,
        out_shape=(jax.ShapeDtypeStruct((ROWS, width), BF16), jax.ShapeDtypeStruct((1, 2, HALF, 2 * HALF), BF16)),
        in_specs=[SMEM] + [VMEM] * 9,
        out_specs=(VMEM, VMEM),
        compiler_params=vmem(16),
        name="front",
    )(place, tokens, up_a, up_b, far_a, far_b, down_a, down_b, norm_gain[None], kv_w)
    kv_oth = lax.ppermute(kv, "c", [(0, 1), (1, 0)])

    beside = [lax.ppermute(kv, "y", ring(4, step)) for step in (1, -1, 2)]
    group = pl.pallas_call(
        join_kernel,
        out_shape=jax.ShapeDtypeStruct((4, 2, HALF, 2 * HALF), BF16),
        in_specs=[VMEM] * 4,
        out_specs=VMEM,
        compiler_params=vmem(8),
        name="join",
    )(kv, *beside)
    columns = (0, -1, 1, 2)
    up, down = [group], [group]
    for k in range(3):
        up.append(lax.ppermute(up[-1], "z", ring(8, 1)))
        down.append(lax.ppermute(down[-1], "z", ring(8, -1)))
    up.append(lax.ppermute(up[3][:2], "z", ring(8, 1)))
    down.append(lax.ppermute(down[3][2:], "z", ring(8, -1)))

    normed, query_weight, kv_oth = lax.optimization_barrier((normed, query_weight, kv_oth))
    query_w = query_weight.reshape(width, -1)
    scale = (query_weight.shape[2] // 2) ** -0.5 * LOG2E
    q_own = (
        lax.dot_general(query_w, normed, (((0,), (1,)), ((), ())), preferred_element_type=F32) * scale
    ).astype(BF16)
    q_oth = lax.ppermute(q_own, "c", [(0, 1), (1, 0)])

    *state, q = pl.pallas_call(
        first_kernel,
        out_shape=(*STATE, pltpu.VMEM((MAPS, 128, 2 * ROWS), BF16)),
        in_specs=[SMEM] + [VMEM] * 4,
        out_specs=(VMEM, VMEM, VMEM),
        scratch_shapes=[pltpu.VMEM((ROWS, 2 * ROWS), BF16)] * 2,
        compiler_params=vmem(16),
        name="first",
    )(place, kv, kv_oth, q_own, q_oth)
    plan = tuple((i, ((0, dy),)) for i, dy in enumerate(columns[1:]))
    state = attend_chunk(place, q, state, plan, beside, "chunk0", rolled=True)
    normed, gate_weight, state = lax.optimization_barrier((normed, gate_weight, state))
    gate_w = gate_weight.reshape(width, -1)
    pool_in = dot(normed, pool_weight[:, 0]).astype(BF16)
    rim = lax.ppermute(pool_in[ROWS - WINDOW :], ("z", "y", "c"), [(i, i + 1) for i in range(63)])
    for k in range(1, 5):
        plan = (
            (0, tuple((-k, dy) for dy in (columns if k < 4 else columns[:2]))),
            (1, tuple((k, dy) for dy in (columns if k < 4 else columns[2:]))),
        )
        state = attend_chunk(place, q, state, plan, (up[k], down[k]), f"chunk{k}", rolled=k == 4)
        if k == 1:
            normed, state = lax.optimization_barrier((normed, state))
            gate_pre = dot(normed, gate_w).astype(BF16)
        if k == 2:
            gate_pre, state = lax.optimization_barrier((gate_pre, state))
            part_shape = jax.ShapeDtypeStruct((ROWS, 512), F32)
            keep, part = pl.pallas_call(
                pool_kernel,
                out_shape=(part_shape, part_shape),
                in_specs=[SMEM] + [VMEM] * 5,
                out_specs=(VMEM, VMEM),
                compiler_params=vmem(16),
                name="pool",
            )(place, pool_in, rim, gate_pre, pool_mix[0], pool_scale)
            state, keep, part = lax.optimization_barrier((state, keep, part))
    other = lax.ppermute(state[1], "c", [(0, 1), (1, 0)])
    piece = jax.ShapeDtypeStruct((32, width), BF16)
    own, up_a, up_b, far_a, far_b, down_a, down_b, logs = pl.pallas_call(
        finish_kernel,
        out_shape=(jax.ShapeDtypeStruct((64, width), BF16), *[piece] * 6, jax.ShapeDtypeStruct((MAPS, ROWS), F32)),
        in_specs=[SMEM, SMEM] + [VMEM] * 6,
        out_specs=(VMEM,) * 8,
        scratch_shapes=[pltpu.VMEM((ROWS, 512), BF16)],
        compiler_params=vmem(24),
        name="finish",
    )(place, mix_lambda, state[0], other, head_gain[None], keep, part, out_weight)
    from_far_a = lax.ppermute(far_a, "x", ring(4, 1))
    from_far_b = lax.ppermute(far_b, "x", ring(4, -1))
    low_b = lax.ppermute(up_b, "x", ring(4, 1))
    high_a = lax.ppermute(down_a, "x", ring(4, -1))

    def add(*arrays):
        return sum(a.astype(F32) for a in arrays).astype(BF16)

    low_a = lax.ppermute(add(up_a, from_far_a), "x", ring(4, 1))
    high_b = lax.ppermute(add(down_b, from_far_b), "x", ring(4, -1))
    mixed = jnp.concatenate([add(own[:32], low_a, high_a), add(own[32:], low_b, high_b)], axis=0)
    return mixed, jnp.transpose(logs.reshape(4, 2, ROWS), (1, 0, 2))


def solution(mesh):
    fine = Mesh(mesh.devices.reshape(8, 4, 2, 4), ("z", "y", "c", "x"))
    sp = ("z", "y", "c")
    in_specs = (
        P((*sp, "x"), None),
        P(),
        P(None, "x", None),
        P(None, "x", None),
        P(None, "x", None),
        P("x"),
        P(),
        P(None, "x", None),
        P("x", None, None),
        P("x", None),
        P(None, None, "x"),
        P("x", None),
    )
    out_specs = (P((*sp, "x"), None), P(None, "x", sp))
    return jax.shard_map(local, mesh=fine, in_specs=in_specs, out_specs=out_specs, check_vma=False)
```

```python
import functools
import math

import jax
import jax.numpy as jnp
from jax import lax
from jax.experimental import pallas as pl
from jax.experimental.pallas import tpu as pltpu
from jax.sharding import Mesh
from jax.sharding import PartitionSpec as P


NORM_EPS = 1e-06
WINDOW = 16
ROWS = 256
HALF = 128
MAPS = 8
ST = 152
NEG = -1e30
LIMIT = 64.0
LOG2E = math.log2(math.e)
VMEM = pl.BlockSpec(memory_space=pltpu.VMEM)
SMEM = pl.BlockSpec(memory_space=pltpu.SMEM)
F32 = jnp.float32
BF16 = jnp.bfloat16


def vmem(mib):
    return pltpu.CompilerParams(vmem_limit_bytes=mib << 20)


def ring(size, step):
    return [(i, (i + step) % size) for i in range(size)]


def dot(a, b):
    return jnp.dot(a, b, preferred_element_type=F32)


def with_ones(v0, v1):
    values = jnp.concatenate([v0, v1], axis=1)
    return jnp.concatenate([values, jnp.ones((16, values.shape[1]), BF16)], axis=0)


def first_kernel(place_ref, kv_ref, oth_kv_ref, q_own_ref, q_oth_ref, own_ref, oth_ref, q_ref, p_a, p_b):
    for i in range(MAPS):
        here, there = slice(i % 2 * 64, i % 2 * 64 + 64), slice(64 - i % 2 * 64, 128 - i % 2 * 64)
        q_ref[i, here, :ROWS] = q_own_ref[i * 64 : i * 64 + 64]
        q_ref[i, here, ROWS:] = q_oth_ref[i * 64 : i * 64 + 64]
        q_ref[i, there] = jnp.zeros((64, 2 * ROWS), BF16)
    keys = jnp.concatenate([kv_ref[0, 0, :, :HALF], kv_ref[0, 1, :, :HALF]], axis=0)
    oth_keys = jnp.concatenate([oth_kv_ref[0, 0, :, :HALF], oth_kv_ref[0, 1, :, :HALF]], axis=0)
    values = with_ones(kv_ref[0, 0, :, HALF:], kv_ref[0, 1, :, HALF:])
    row = lax.broadcasted_iota(jnp.int32, (ROWS, 2 * ROWS), 0)
    col = lax.broadcasted_iota(jnp.int32, (ROWS, 2 * ROWS), 1)
    seen = row <= jnp.where(col < ROWS, col, jnp.where(place_ref[2] == 0, ROWS, -1))
    diagonal = (row <= col)[:, :ROWS]
    probs = (p_a, p_b)

    def scores(i, slot):
        s = jnp.where(seen, dot(keys, q_ref[i]), NEG)
        seed = jnp.max(jnp.where(diagonal, dot(oth_keys, q_ref[i, :, ROWS:]), NEG), axis=0, keepdims=True)
        top = jnp.max(s, axis=0, keepdims=True)
        top = jnp.concatenate([top[:, :ROWS], jnp.maximum(top[:, ROWS:], seed)], axis=1)
        probs[slot][...] = jnp.exp2(s - top).astype(BF16)
        own_ref[i, 144:152] = jnp.broadcast_to(top[:, :ROWS], (8, ROWS))
        oth_ref[i, 144:152] = jnp.broadcast_to(top[:, ROWS:], (8, ROWS))

    def sums(i, slot):
        out = dot(values, probs[slot][...])
        own_ref[i, 0:144] = out[:, :ROWS]
        oth_ref[i, 0:144] = out[:, ROWS:]

    def two_maps(h, carry):
        scores(2 * h, 0)
        scores(2 * h + 1, 1)
        sums(2 * h, 0)
        sums(2 * h + 1, 1)
        return carry

    lax.fori_loop(0, MAPS // 2, two_maps, 0)


def join_kernel(a, b, c, d, out_ref):
    for i, ref in enumerate((a, b, c, d)):
        out_ref[i] = ref[0]


def front_kernel(place_ref, p0, p1a, p1b, p2a, p2b, p3a, p3b, gain_ref, w_ref, normed_ref, kv_ref):
    x = place_ref[3]

    def put(piece_ref, back, half, rows):
        values = piece_ref[...].astype(F32)
        scale = lax.rsqrt(jnp.mean(values * values, axis=1, keepdims=True) + NORM_EPS)
        at = pl.multiple_of(((x - back) & 3) * 64 + half * 32, 32)
        normed_ref[pl.ds(at, rows), :] = (values * scale * gain_ref[...]).astype(BF16)

    put(p0, 0, 0, 64)
    put(p1a, 1, 0, 32)
    put(p1b, 1, 1, 32)
    put(p3a, 3, 0, 32)
    put(p3b, 3, 1, 32)
    put(p2a, 2, 0, 32)
    put(p2b, 2, 1, 32)
    both = dot(normed_ref[...], w_ref[...])
    values_t = both[:, HALF:].T.astype(BF16)
    for half in range(2):
        rows = slice(half * HALF, half * HALF + HALF)
        kv_ref[0, half, :, :HALF] = both[rows, :HALF].astype(BF16)
        kv_ref[0, half, :, HALF:] = values_t[:, rows]


def chunk_kernel(plan, n_in, rolled, *refs):
    place_ref, q_ref = refs[0], refs[1]
    ins = refs[2 : 2 + n_in]
    own_in, oth_in, own_ref, oth_ref, keys_ref, values_ref, p_a, p_b, over_ref, list_ref = refs[2 + n_in :]
    probs = (p_a, p_b)
    z, y = place_ref[0], place_ref[1]
    visible = jnp.int32(0)
    at = 0
    for _, offsets in plan:
        for dz, dy in offsets:
            sees = ((z + dz) & 7) * 4 + ((y + dy) & 3) < z * 4 + y
            list_ref[visible] = at
            visible = visible + sees.astype(jnp.int32)
            at += 1

    def fetch(which, slot):
        at = 0
        rows = slice(slot * ROWS, slot * ROWS + HALF), slice(slot * ROWS + HALF, slot * ROWS + ROWS)
        for pair, offsets in plan:
            count = len(offsets)

            @pl.when((which >= at) & (which < at + count))
            def _(pair=pair, at=at):
                b = which - at
                for half in range(2):
                    source = ins[pair].at[b, half]
                    keys_ref[rows[half]] = source[:, :HALF]
                    values_ref[0:HALF, rows[half]] = source[:, HALF:]

            at += count

    def keep_state():
        own_ref[...] = own_in[...]
        oth_ref[...] = oth_in[...]

    pl.when(visible == 0)(keep_state)

    @pl.when(visible > 0)
    def _():
        own_ref[:, 144:] = own_in[:, 144:]
        oth_ref[:, 144:] = oth_in[:, 144:]
        over_ref[...] = jnp.full(over_ref.shape, NEG, F32)
        values_ref[HALF:144] = jnp.ones((16, 2 * ROWS), BF16)

        def two_blocks(t, carry):
            fetch(list_ref[2 * t], 0)
            second = 2 * t + 1 < visible
            fetch(list_ref[jnp.minimum(2 * t + 1, visible - 1)], 1)

            @pl.when(jnp.logical_not(second))
            def _():
                values_ref[:, ROWS:] = jnp.zeros((144, ROWS), BF16)

            keys, values = keys_ref[...], values_ref[...]

            def scores(i, slot):
                top = jnp.concatenate([own_in[i, 144:145], oth_in[i, 144:145]], axis=1)
                s = dot(keys, q_ref[i]) - top
                over_ref[i] = jnp.maximum(over_ref[i], jnp.max(s.reshape(-1, 8, 2 * ROWS), axis=0))
                probs[slot][...] = jnp.exp2(s).astype(BF16)

            def sums(i, slot):
                out = dot(values, probs[slot][...])
                own_ref[i, 0:144] = jnp.where(t == 0, own_in[i, 0:144], own_ref[i, 0:144]) + out[:, :ROWS]
                oth_ref[i, 0:144] = jnp.where(t == 0, oth_in[i, 0:144], oth_ref[i, 0:144]) + out[:, ROWS:]

            def two_maps(h, carry):
                scores(2 * h, 0)
                scores(2 * h + 1, 1)
                sums(2 * h, 0)
                sums(2 * h + 1, 1)
                return carry

            if rolled:
                return lax.fori_loop(0, MAPS // 2, two_maps, carry)
            scores(0, 0)
            for i in range(MAPS):
                if i + 1 < MAPS:
                    scores(i + 1, (i + 1) % 2)
                sums(i, i % 2)
            return carry

        lax.fori_loop(0, (visible + 1) // 2, two_blocks, 0)

        @pl.when(jnp.logical_not(jnp.max(over_ref[...]) <= LIMIT))
        def _():
            keep_state()
            values_ref[HALF:144] = jnp.ones((16, 2 * ROWS), BF16)

            def one_block(t, carry):
                fetch(list_ref[t], 0)

                def one_map(i, carry):
                    before = jnp.concatenate([own_ref[i, 144:145], oth_ref[i, 144:145]], axis=1)
                    s = dot(keys_ref[:ROWS], q_ref[i])
                    top = jnp.maximum(before, jnp.max(s, axis=0, keepdims=True))
                    scale = jnp.exp2(before - top)
                    out = dot(values_ref[:, :ROWS], jnp.exp2(s - top).astype(BF16))
                    top8 = jnp.broadcast_to(top, (8, 2 * ROWS))
                    own_ref[i, 0:144] = own_ref[i, 0:144] * scale[:, :ROWS] + out[:, :ROWS]
                    oth_ref[i, 0:144] = oth_ref[i, 0:144] * scale[:, ROWS:] + out[:, ROWS:]
                    own_ref[i, 144:152] = top8[:, :ROWS]
                    oth_ref[i, 144:152] = top8[:, ROWS:]
                    return carry

                return lax.fori_loop(0, MAPS, one_map, carry)

            lax.fori_loop(0, visible, one_block, 0)


STATE = (pltpu.VMEM((MAPS, ST, ROWS), F32), pltpu.VMEM((MAPS, ST, ROWS), F32))


def in_vmem(array):
    return pltpu.with_memory_space_constraint(array, pltpu.VMEM)


def attend_chunk(place, q, state, plan, arrays, rolled=False):
    n = len(arrays)
    blocks = sum(len(offsets) for _, offsets in plan)
    return pl.pallas_call(
        functools.partial(chunk_kernel, plan, n, rolled),
        out_shape=STATE,
        in_specs=[SMEM, VMEM] + [VMEM] * n + [VMEM, VMEM],
        out_specs=(VMEM, VMEM),
        scratch_shapes=[
            pltpu.VMEM((2 * ROWS, HALF), BF16),
            pltpu.VMEM((144, 2 * ROWS), BF16),
            pltpu.VMEM((2 * ROWS, 2 * ROWS), BF16),
            pltpu.VMEM((2 * ROWS, 2 * ROWS), BF16),
            pltpu.VMEM((MAPS, 8, 2 * ROWS), F32),
            pltpu.SMEM((blocks + 1,), jnp.int32),
        ],
        cost_estimate=pl.CostEstimate(
            flops=blocks * MAPS * 2 * 256 * 512 * 512, transcendentals=blocks * MAPS * 256 * 512, bytes_accessed=1 << 20
        ),
        compiler_params=vmem(20),
    )(place, in_vmem(q), *arrays, in_vmem(state[0]), in_vmem(state[1]))


def pool_kernel(place_ref, pool_ref, rim_ref, gate_ref, mix_ref, scale_ref, keep_ref, part_ref):
    span = jnp.left_shift(jnp.int32(2), place_ref[3])
    start = ((place_ref[0] * 4 + place_ref[1]) * 2 + place_ref[2]) * ROWS
    now = pool_ref[...].astype(F32)
    sums = jnp.concatenate([rim_ref[...].astype(F32), now], axis=0)
    rows = WINDOW + ROWS
    picked = jnp.zeros((ROWS, now.shape[1]), F32)
    for width in (1, 2, 4, 8):
        sums = sums + jnp.concatenate([jnp.zeros((width, now.shape[1]), F32), sums[: rows - width]], axis=0)
        picked = jnp.where(span == 2 * width, sums[WINDOW:], picked)
    position = start + lax.broadcasted_iota(jnp.int32, (ROWS, 1), 0)
    counts = jnp.minimum(position + 1, span).astype(F32)
    pooled = (picked / counts - now).astype(BF16)
    mixed = dot(pooled, mix_ref[...]) * scale_ref[...]
    width = now.shape[1]
    keep_ref[...] = jax.nn.sigmoid(gate_ref[:, :width].astype(F32))
    part_ref[...] = jax.nn.sigmoid(gate_ref[:, width:].astype(F32)) * mixed


def finish_kernel(place_ref, lam_ref, a_ref, b_ref, gain_ref, keep_ref, part_ref, w_ref, *refs):
    own_out, up_a, up_b, far_a, far_b, down_a, down_b, log_ref, merged_ref = refs
    x = place_ref[3]
    for h in range(MAPS // 2):
        maps = []
        for m in range(2):
            i = 2 * h + m
            top_a, top_b = a_ref[i, 144:145], b_ref[i, 144:145]
            top = jnp.maximum(top_a, top_b)
            wa, wb = jnp.exp2(top_a - top), jnp.exp2(top_b - top)
            total = a_ref[i, 128:129] * wa + b_ref[i, 128:129] * wb
            log_ref[i : i + 1, :] = (top + jnp.log2(total)) * (1.0 / LOG2E)
            maps.append((a_ref[i, 0:128] * wa + b_ref[i, 0:128] * wb) / total)
        head = maps[0] - lam_ref[h] * maps[1]
        head = head * lax.rsqrt(jnp.mean(head * head, axis=0, keepdims=True) + NORM_EPS)
        cols = slice(h * 128, h * 128 + 128)
        merged = (keep_ref[:, cols] * (head.T * gain_ref[...]) + part_ref[:, cols]).astype(BF16)
        for j in range(4):
            at = pl.multiple_of(((j - x) & 3) * 64, 64)
            merged_ref[pl.ds(at, 64), cols] = merged[j * 64 : j * 64 + 64]
    out = dot(merged_ref[...], w_ref[...]).astype(BF16)
    own_out[...] = out[:64]
    for i, ref in enumerate((up_a, up_b, far_a, far_b, down_a, down_b)):
        ref[...] = out[64 + i * 32 : 96 + i * 32]


def local(tokens, norm_gain, query_weight, key_weight, value_weight, mix_lambda, head_gain, pool_weight, pool_mix, pool_scale, gate_weight, out_weight):
    width = tokens.shape[1]
    z, y, c = lax.axis_index("z"), lax.axis_index("y"), lax.axis_index("c")
    place = jnp.stack([z, y, c, lax.axis_index("x")])
    halves = tokens[:32], tokens[32:]
    up_a = lax.ppermute(halves[0], "x", ring(4, 1))
    down_b = lax.ppermute(halves[1], "x", ring(4, -1))
    up_b = lax.ppermute(halves[1], "x", ring(4, 1))
    down_a = lax.ppermute(halves[0], "x", ring(4, -1))
    far_a = lax.ppermute(up_a, "x", ring(4, 1))
    far_b = lax.ppermute(down_b, "x", ring(4, -1))
    kv_w = jnp.concatenate([key_weight[:, 0], value_weight[:, 0]], axis=1)
    normed, kv = pl.pallas_call(
        front_kernel,
        out_shape=(jax.ShapeDtypeStruct((ROWS, width), BF16), jax.ShapeDtypeStruct((1, 2, HALF, 2 * HALF), BF16)),
        in_specs=[SMEM] + [VMEM] * 9,
        out_specs=(VMEM, VMEM),
        compiler_params=vmem(16),
        name="front",
    )(place, tokens, up_a, up_b, far_a, far_b, down_a, down_b, norm_gain[None], kv_w)
    kv_oth = lax.ppermute(kv, "c", [(0, 1), (1, 0)])

    beside = []
    for step in (1, -1, 2):
        beside.append(lax.ppermute(kv, "y", ring(4, step)))
    group = pl.pallas_call(
        join_kernel,
        out_shape=jax.ShapeDtypeStruct((4, 2, HALF, 2 * HALF), BF16),
        in_specs=[VMEM] * 4,
        out_specs=VMEM,
        compiler_params=vmem(8),
        name="join",
    )(kv, *beside)
    columns = (0, -1, 1, 2)
    up, down = [group], [group]
    for k in range(3):
        up.append(lax.ppermute(up[-1], "z", ring(8, 1)))
        down.append(lax.ppermute(down[-1], "z", ring(8, -1)))
    up.append(lax.ppermute(up[3][:2], "z", ring(8, 1)))
    down.append(lax.ppermute(down[3][2:], "z", ring(8, -1)))

    scale = (query_weight.shape[2] // 2) ** -0.5 * LOG2E
    query_w = query_weight.reshape(width, -1)
    q_own = (
        lax.dot_general(query_w, normed, (((0,), (1,)), ((), ())), preferred_element_type=F32) * scale
    ).astype(BF16)
    q_oth = lax.ppermute(q_own, "c", [(0, 1), (1, 0)])

    *state, q = pl.pallas_call(
        first_kernel,
        out_shape=(*STATE, pltpu.VMEM((MAPS, 128, 2 * ROWS), BF16)),
        in_specs=[SMEM] + [VMEM] * 4,
        out_specs=(VMEM, VMEM, VMEM),
        scratch_shapes=[pltpu.VMEM((ROWS, 2 * ROWS), BF16)] * 2,
        compiler_params=vmem(16),
        name="first",
    )(place, kv, kv_oth, q_own, q_oth)
    plan = tuple((i, ((0, dy),)) for i, dy in enumerate(columns[1:]))
    state = attend_chunk(place, q, state, plan, beside, rolled=True)
    normed, gate_weight, state = lax.optimization_barrier((normed, gate_weight, state))
    gate_w = gate_weight.reshape(width, -1)
    pool_in = dot(normed, pool_weight[:, 0]).astype(BF16)
    rim = lax.ppermute(pool_in[ROWS - WINDOW :], ("z", "y", "c"), [(i, i + 1) for i in range(63)])
    for k in range(1, 5):
        plan = (
            (0, tuple((-k, dy) for dy in (columns if k < 4 else columns[:2]))),
            (1, tuple((k, dy) for dy in (columns if k < 4 else columns[2:]))),
        )
        state = attend_chunk(place, q, state, plan, (up[k], down[k]), rolled=k == 4)
        if k == 1:
            normed, state = lax.optimization_barrier((normed, state))
            gate_pre = dot(normed, gate_w).astype(BF16)
        if k == 2:
            gate_pre, state = lax.optimization_barrier((gate_pre, state))
            part_shape = jax.ShapeDtypeStruct((ROWS, 512), F32)
            keep, part = pl.pallas_call(
                pool_kernel,
                out_shape=(part_shape, part_shape),
                in_specs=[SMEM] + [VMEM] * 5,
                out_specs=(VMEM, VMEM),
                compiler_params=vmem(16),
                name="pool",
            )(place, pool_in, rim, gate_pre, pool_mix[0], pool_scale)
            state, keep, part = lax.optimization_barrier((state, keep, part))
    other = lax.ppermute(state[1], "c", [(0, 1), (1, 0)])
    piece = jax.ShapeDtypeStruct((32, width), BF16)
    own, up_a, up_b, far_a, far_b, down_a, down_b, logs = pl.pallas_call(
        finish_kernel,
        out_shape=(jax.ShapeDtypeStruct((64, width), BF16), *[piece] * 6, jax.ShapeDtypeStruct((MAPS, ROWS), F32)),
        in_specs=[SMEM, SMEM] + [VMEM] * 6,
        out_specs=(VMEM,) * 8,
        scratch_shapes=[pltpu.VMEM((ROWS, 512), BF16)],
        compiler_params=vmem(24),
        name="finish",
    )(place, mix_lambda, state[0], other, head_gain[None], keep, part, out_weight)
    from_far_a = lax.ppermute(far_a, "x", ring(4, 1))
    from_far_b = lax.ppermute(far_b, "x", ring(4, -1))
    low_b = lax.ppermute(up_b, "x", ring(4, 1))
    high_a = lax.ppermute(down_a, "x", ring(4, -1))

    def add(*arrays):
        return sum(a.astype(F32) for a in arrays).astype(BF16)

    low_a = lax.ppermute(add(up_a, from_far_a), "x", ring(4, 1))
    high_b = lax.ppermute(add(down_b, from_far_b), "x", ring(4, -1))
    mixed = jnp.concatenate([add(own[:32], low_a, high_a), add(own[32:], low_b, high_b)], axis=0)
    return mixed, jnp.transpose(logs.reshape(4, 2, ROWS), (1, 0, 2))


def solution(mesh):
    fine = Mesh(mesh.devices.reshape(8, 4, 2, 4), ("z", "y", "c", "x"))
    sp = ("z", "y", "c")
    in_specs = (
        P((*sp, "x"), None),
        P(),
        P(None, "x", None),
        P(None, "x", None),
        P(None, "x", None),
        P("x"),
        P(),
        P(None, "x", None),
        P("x", None, None),
        P("x", None),
        P(None, None, "x"),
        P("x", None),
    )
    out_specs = (P((*sp, "x"), None), P(None, "x", sp))
    return jax.shard_map(local, mesh=fine, in_specs=in_specs, out_specs=out_specs, check_vma=False)
```

```python
import functools
import math

import jax
import jax.numpy as jnp
from jax import lax
from jax.experimental import pallas as pl
from jax.experimental.pallas import tpu as pltpu
from jax.sharding import Mesh
from jax.sharding import PartitionSpec as P


NORM_EPS = 1e-06
WINDOW = 16
ROWS = 256
HALF = 128
MAPS = 8
ST = 152
NEG = -1e30
LIMIT = 64.0
LOG2E = math.log2(math.e)
VMEM = pl.BlockSpec(memory_space=pltpu.VMEM)
SMEM = pl.BlockSpec(memory_space=pltpu.SMEM)
F32 = jnp.float32
BF16 = jnp.bfloat16


def vmem(mib):
    return pltpu.CompilerParams(vmem_limit_bytes=mib << 20)


def ring(size, step):
    return [(i, (i + step) % size) for i in range(size)]


def dot(a, b):
    return jnp.dot(a, b, preferred_element_type=F32)


def with_ones(v0, v1):
    values = jnp.concatenate([v0, v1], axis=1)
    return jnp.concatenate([values, jnp.ones((16, values.shape[1]), BF16)], axis=0)


def first_kernel(place_ref, kv_ref, oth_kv_ref, q_own_ref, q_oth_ref, own_ref, oth_ref, q_ref, p_a, p_b):
    for i in range(MAPS):
        here, there = slice(i % 2 * 64, i % 2 * 64 + 64), slice(64 - i % 2 * 64, 128 - i % 2 * 64)
        q_ref[i, here, :ROWS] = q_own_ref[i * 64 : i * 64 + 64]
        q_ref[i, here, ROWS:] = q_oth_ref[i * 64 : i * 64 + 64]
        q_ref[i, there] = jnp.zeros((64, 2 * ROWS), BF16)
    keys = jnp.concatenate([kv_ref[0, 0, :, :HALF], kv_ref[0, 1, :, :HALF]], axis=0)
    oth_keys = jnp.concatenate([oth_kv_ref[0, 0, :, :HALF], oth_kv_ref[0, 1, :, :HALF]], axis=0)
    values = with_ones(kv_ref[0, 0, :, HALF:], kv_ref[0, 1, :, HALF:])
    row = lax.broadcasted_iota(jnp.int32, (ROWS, 2 * ROWS), 0)
    col = lax.broadcasted_iota(jnp.int32, (ROWS, 2 * ROWS), 1)
    seen = row <= jnp.where(col < ROWS, col, jnp.where(place_ref[2] == 0, ROWS, -1))
    diagonal = (row <= col)[:, :ROWS]
    probs = (p_a, p_b)

    def scores(i, slot):
        s = jnp.where(seen, dot(keys, q_ref[i]), NEG)
        seed = jnp.max(jnp.where(diagonal, dot(oth_keys, q_ref[i, :, ROWS:]), NEG), axis=0, keepdims=True)
        top = jnp.max(s, axis=0, keepdims=True)
        top = jnp.concatenate([top[:, :ROWS], jnp.maximum(top[:, ROWS:], seed)], axis=1)
        probs[slot][...] = jnp.exp2(s - top).astype(BF16)
        own_ref[i, 144:152] = jnp.broadcast_to(top[:, :ROWS], (8, ROWS))
        oth_ref[i, 144:152] = jnp.broadcast_to(top[:, ROWS:], (8, ROWS))

    def sums(i, slot):
        out = dot(values, probs[slot][...])
        own_ref[i, 0:144] = out[:, :ROWS]
        oth_ref[i, 0:144] = out[:, ROWS:]

    def two_maps(h, carry):
        scores(2 * h, 0)
        scores(2 * h + 1, 1)
        sums(2 * h, 0)
        sums(2 * h + 1, 1)
        return carry

    lax.fori_loop(0, MAPS // 2, two_maps, 0)


def join_kernel(a, b, c, d, out_ref):
    for i, ref in enumerate((a, b, c, d)):
        out_ref[i] = ref[0]


def front_kernel(place_ref, p0, p1a, p1b, p2a, p2b, p3a, p3b, gain_ref, w_ref, normed_ref, kv_ref):
    x = place_ref[3]

    def put(piece_ref, back, half, rows):
        values = piece_ref[...].astype(F32)
        scale = lax.rsqrt(jnp.mean(values * values, axis=1, keepdims=True) + NORM_EPS)
        at = pl.multiple_of(((x - back) & 3) * 64 + half * 32, 32)
        normed_ref[pl.ds(at, rows), :] = (values * scale * gain_ref[...]).astype(BF16)

    put(p0, 0, 0, 64)
    put(p1a, 1, 0, 32)
    put(p1b, 1, 1, 32)
    put(p3a, 3, 0, 32)
    put(p3b, 3, 1, 32)
    put(p2a, 2, 0, 32)
    put(p2b, 2, 1, 32)
    both = dot(normed_ref[...], w_ref[...])
    values_t = both[:, HALF:].T.astype(BF16)
    for half in range(2):
        rows = slice(half * HALF, half * HALF + HALF)
        kv_ref[0, half, :, :HALF] = both[rows, :HALF].astype(BF16)
        kv_ref[0, half, :, HALF:] = values_t[:, rows]


def chunk_kernel(plan, n_in, rolled, *refs):
    place_ref, q_ref = refs[0], refs[1]
    ins = refs[2 : 2 + n_in]
    own_in, oth_in, own_ref, oth_ref, keys_ref, values_ref, p_a, p_b, over_ref, list_ref = refs[2 + n_in :]
    probs = (p_a, p_b)
    z, y = place_ref[0], place_ref[1]
    visible = jnp.int32(0)
    at = 0
    for _, offsets in plan:
        for dz, dy in offsets:
            sees = ((z + dz) & 7) * 4 + ((y + dy) & 3) < z * 4 + y
            list_ref[visible] = at
            visible = visible + sees.astype(jnp.int32)
            at += 1

    def fetch(which, slot):
        at = 0
        rows = slice(slot * ROWS, slot * ROWS + HALF), slice(slot * ROWS + HALF, slot * ROWS + ROWS)
        for pair, offsets in plan:
            count = len(offsets)

            @pl.when((which >= at) & (which < at + count))
            def _(pair=pair, at=at):
                b = which - at
                for half in range(2):
                    source = ins[pair].at[b, half]
                    keys_ref[rows[half]] = source[:, :HALF]
                    values_ref[0:HALF, rows[half]] = source[:, HALF:]

            at += count

    def keep_state():
        own_ref[...] = own_in[...]
        oth_ref[...] = oth_in[...]

    pl.when(visible == 0)(keep_state)

    @pl.when(visible > 0)
    def _():
        own_ref[:, 144:] = own_in[:, 144:]
        oth_ref[:, 144:] = oth_in[:, 144:]
        over_ref[...] = jnp.full(over_ref.shape, NEG, F32)
        values_ref[HALF:144] = jnp.ones((16, 2 * ROWS), BF16)

        def two_blocks(t, carry):
            fetch(list_ref[2 * t], 0)
            second = 2 * t + 1 < visible
            fetch(list_ref[jnp.minimum(2 * t + 1, visible - 1)], 1)

            @pl.when(jnp.logical_not(second))
            def _():
                values_ref[:, ROWS:] = jnp.zeros((144, ROWS), BF16)

            keys, values = keys_ref[...], values_ref[...]

            def scores(i, slot):
                top = jnp.concatenate([own_in[i, 144:145], oth_in[i, 144:145]], axis=1)
                s = dot(keys, q_ref[i]) - top
                over_ref[i] = jnp.maximum(over_ref[i], jnp.max(s.reshape(-1, 8, 2 * ROWS), axis=0))
                probs[slot][...] = jnp.exp2(s).astype(BF16)

            def sums(i, slot):
                out = dot(values, probs[slot][...])
                own_ref[i, 0:144] = jnp.where(t == 0, own_in[i, 0:144], own_ref[i, 0:144]) + out[:, :ROWS]
                oth_ref[i, 0:144] = jnp.where(t == 0, oth_in[i, 0:144], oth_ref[i, 0:144]) + out[:, ROWS:]

            def two_maps(h, carry):
                scores(2 * h, 0)
                scores(2 * h + 1, 1)
                sums(2 * h, 0)
                sums(2 * h + 1, 1)
                return carry

            if rolled:
                return lax.fori_loop(0, MAPS // 2, two_maps, carry)
            scores(0, 0)
            for i in range(MAPS):
                if i + 1 < MAPS:
                    scores(i + 1, (i + 1) % 2)
                sums(i, i % 2)
            return carry

        lax.fori_loop(0, (visible + 1) // 2, two_blocks, 0)

        @pl.when(jnp.logical_not(jnp.max(over_ref[...]) <= LIMIT))
        def _():
            keep_state()
            values_ref[HALF:144] = jnp.ones((16, 2 * ROWS), BF16)

            def one_block(t, carry):
                fetch(list_ref[t], 0)

                def one_map(i, carry):
                    before = jnp.concatenate([own_ref[i, 144:145], oth_ref[i, 144:145]], axis=1)
                    s = dot(keys_ref[:ROWS], q_ref[i])
                    top = jnp.maximum(before, jnp.max(s, axis=0, keepdims=True))
                    scale = jnp.exp2(before - top)
                    out = dot(values_ref[:, :ROWS], jnp.exp2(s - top).astype(BF16))
                    top8 = jnp.broadcast_to(top, (8, 2 * ROWS))
                    own_ref[i, 0:144] = own_ref[i, 0:144] * scale[:, :ROWS] + out[:, :ROWS]
                    oth_ref[i, 0:144] = oth_ref[i, 0:144] * scale[:, ROWS:] + out[:, ROWS:]
                    own_ref[i, 144:152] = top8[:, :ROWS]
                    oth_ref[i, 144:152] = top8[:, ROWS:]
                    return carry

                return lax.fori_loop(0, MAPS, one_map, carry)

            lax.fori_loop(0, visible, one_block, 0)


STATE = (pltpu.VMEM((MAPS, ST, ROWS), F32), pltpu.VMEM((MAPS, ST, ROWS), F32))


def in_vmem(array):
    return pltpu.with_memory_space_constraint(array, pltpu.VMEM)


def attend_chunk(place, q, state, plan, arrays, rolled=False):
    n = len(arrays)
    blocks = sum(len(offsets) for _, offsets in plan)
    return pl.pallas_call(
        functools.partial(chunk_kernel, plan, n, rolled),
        out_shape=STATE,
        in_specs=[SMEM, VMEM] + [VMEM] * n + [VMEM, VMEM],
        out_specs=(VMEM, VMEM),
        scratch_shapes=[
            pltpu.VMEM((2 * ROWS, HALF), BF16),
            pltpu.VMEM((144, 2 * ROWS), BF16),
            pltpu.VMEM((2 * ROWS, 2 * ROWS), BF16),
            pltpu.VMEM((2 * ROWS, 2 * ROWS), BF16),
            pltpu.VMEM((MAPS, 8, 2 * ROWS), F32),
            pltpu.SMEM((blocks + 1,), jnp.int32),
        ],
        cost_estimate=pl.CostEstimate(
            flops=blocks * MAPS * 2 * 256 * 512 * 512, transcendentals=blocks * MAPS * 256 * 512, bytes_accessed=1 << 20
        ),
        compiler_params=vmem(20),
    )(place, in_vmem(q), *arrays, in_vmem(state[0]), in_vmem(state[1]))


def pool_kernel(place_ref, pool_ref, rim_ref, gate_ref, mix_ref, scale_ref, keep_ref, part_ref):
    span = jnp.left_shift(jnp.int32(2), place_ref[3])
    start = ((place_ref[0] * 4 + place_ref[1]) * 2 + place_ref[2]) * ROWS
    now = pool_ref[...].astype(F32)
    sums = jnp.concatenate([rim_ref[...].astype(F32), now], axis=0)
    rows = WINDOW + ROWS
    picked = jnp.zeros((ROWS, now.shape[1]), F32)
    for width in (1, 2, 4, 8):
        sums = sums + jnp.concatenate([jnp.zeros((width, now.shape[1]), F32), sums[: rows - width]], axis=0)
        picked = jnp.where(span == 2 * width, sums[WINDOW:], picked)
    position = start + lax.broadcasted_iota(jnp.int32, (ROWS, 1), 0)
    counts = jnp.minimum(position + 1, span).astype(F32)
    pooled = (picked / counts - now).astype(BF16)
    mixed = dot(pooled, mix_ref[...]) * scale_ref[...]
    width = now.shape[1]
    keep_ref[...] = jax.nn.sigmoid(gate_ref[:, :width].astype(F32))
    part_ref[...] = jax.nn.sigmoid(gate_ref[:, width:].astype(F32)) * mixed


def finish_kernel(place_ref, lam_ref, a_ref, b_ref, gain_ref, keep_ref, part_ref, w_ref, *refs):
    own_out, up_a, up_b, far_a, far_b, down_a, down_b, log_ref, merged_ref = refs
    x = place_ref[3]
    for h in range(MAPS // 2):
        maps = []
        for m in range(2):
            i = 2 * h + m
            top_a, top_b = a_ref[i, 144:145], b_ref[i, 144:145]
            top = jnp.maximum(top_a, top_b)
            wa, wb = jnp.exp2(top_a - top), jnp.exp2(top_b - top)
            total = a_ref[i, 128:129] * wa + b_ref[i, 128:129] * wb
            log_ref[i : i + 1, :] = (top + jnp.log2(total)) * (1.0 / LOG2E)
            maps.append((a_ref[i, 0:128] * wa + b_ref[i, 0:128] * wb) / total)
        head = maps[0] - lam_ref[h] * maps[1]
        head = head * lax.rsqrt(jnp.mean(head * head, axis=0, keepdims=True) + NORM_EPS)
        cols = slice(h * 128, h * 128 + 128)
        merged = (keep_ref[:, cols] * (head.T * gain_ref[...]) + part_ref[:, cols]).astype(BF16)
        for j in range(4):
            at = pl.multiple_of(((j - x) & 3) * 64, 64)
            merged_ref[pl.ds(at, 64), cols] = merged[j * 64 : j * 64 + 64]
    out = dot(merged_ref[...], w_ref[...]).astype(BF16)
    own_out[...] = out[:64]
    for i, ref in enumerate((up_a, up_b, far_a, far_b, down_a, down_b)):
        ref[...] = out[64 + i * 32 : 96 + i * 32]


def local(tokens, norm_gain, query_weight, key_weight, value_weight, mix_lambda, head_gain, pool_weight, pool_mix, pool_scale, gate_weight, out_weight):
    width = tokens.shape[1]
    z, y, c = lax.axis_index("z"), lax.axis_index("y"), lax.axis_index("c")
    place = jnp.stack([z, y, c, lax.axis_index("x")])
    halves = tokens[:32], tokens[32:]
    up_a = lax.ppermute(halves[0], "x", ring(4, 1))
    down_b = lax.ppermute(halves[1], "x", ring(4, -1))
    up_b = lax.ppermute(halves[1], "x", ring(4, 1))
    down_a = lax.ppermute(halves[0], "x", ring(4, -1))
    far_a = lax.ppermute(up_a, "x", ring(4, 1))
    far_b = lax.ppermute(down_b, "x", ring(4, -1))
    kv_w = jnp.concatenate([key_weight[:, 0], value_weight[:, 0]], axis=1)
    normed, kv = pl.pallas_call(
        front_kernel,
        out_shape=(jax.ShapeDtypeStruct((ROWS, width), BF16), jax.ShapeDtypeStruct((1, 2, HALF, 2 * HALF), BF16)),
        in_specs=[SMEM] + [VMEM] * 9,
        out_specs=(VMEM, VMEM),
        compiler_params=vmem(16),
        name="front",
    )(place, tokens, up_a, up_b, far_a, far_b, down_a, down_b, norm_gain[None], kv_w)
    kv_oth = lax.ppermute(kv, "c", [(0, 1), (1, 0)])

    beside = []
    for step in (1, -1, 2):
        beside.append(lax.ppermute(kv, "y", ring(4, step)))
    group = pl.pallas_call(
        join_kernel,
        out_shape=jax.ShapeDtypeStruct((4, 2, HALF, 2 * HALF), BF16),
        in_specs=[VMEM] * 4,
        out_specs=VMEM,
        compiler_params=vmem(8),
        name="join",
    )(kv, *beside)
    columns = (0, -1, 1, 2)
    up, down = [group], [group]
    for k in range(3):
        up.append(lax.ppermute(up[-1], "z", ring(8, 1)))
        down.append(lax.ppermute(down[-1], "z", ring(8, -1)))
    up.append(lax.ppermute(up[3][:2], "z", ring(8, 1)))
    down.append(lax.ppermute(down[3][2:], "z", ring(8, -1)))

    scale = (query_weight.shape[2] // 2) ** -0.5 * LOG2E
    query_w = query_weight.reshape(width, -1)
    q_own = (
        lax.dot_general(query_w, normed, (((0,), (1,)), ((), ())), preferred_element_type=F32) * scale
    ).astype(BF16)
    q_oth = lax.ppermute(q_own, "c", [(0, 1), (1, 0)])

    pool_in = dot(normed, pool_weight[:, 0]).astype(BF16)
    rim = lax.ppermute(pool_in[ROWS - WINDOW :], ("z", "y", "c"), [(i, i + 1) for i in range(63)])
    gate_weight, pool_in = lax.optimization_barrier((gate_weight, pool_in))
    gate_w = gate_weight.reshape(width, -1)
    q_own, gate_w = lax.optimization_barrier((q_own, gate_w))

    *state, q = pl.pallas_call(
        first_kernel,
        out_shape=(*STATE, pltpu.VMEM((MAPS, 128, 2 * ROWS), BF16)),
        in_specs=[SMEM] + [VMEM] * 4,
        out_specs=(VMEM, VMEM, VMEM),
        scratch_shapes=[pltpu.VMEM((ROWS, 2 * ROWS), BF16)] * 2,
        compiler_params=vmem(16),
        name="first",
    )(place, kv, kv_oth, q_own, q_oth)
    plan = tuple((i, ((0, dy),)) for i, dy in enumerate(columns[1:]))
    state = attend_chunk(place, q, state, plan, beside, rolled=True)
    for k in range(1, 5):
        plan = (
            (0, tuple((-k, dy) for dy in (columns if k < 4 else columns[:2]))),
            (1, tuple((k, dy) for dy in (columns if k < 4 else columns[2:]))),
        )
        state = attend_chunk(place, q, state, plan, (up[k], down[k]))
    other = lax.ppermute(state[1], "c", [(0, 1), (1, 0)])
    normed, mine = lax.optimization_barrier((normed, state[0]))
    gate_pre = dot(normed, gate_w).astype(BF16)
    part_shape = jax.ShapeDtypeStruct((ROWS, 512), F32)
    keep, part = pl.pallas_call(
        pool_kernel,
        out_shape=(part_shape, part_shape),
        in_specs=[SMEM] + [VMEM] * 5,
        out_specs=(VMEM, VMEM),
        compiler_params=vmem(16),
        name="pool",
    )(place, pool_in, rim, gate_pre, pool_mix[0], pool_scale)
    piece = jax.ShapeDtypeStruct((32, width), BF16)
    own, up_a, up_b, far_a, far_b, down_a, down_b, logs = pl.pallas_call(
        finish_kernel,
        out_shape=(jax.ShapeDtypeStruct((64, width), BF16), *[piece] * 6, jax.ShapeDtypeStruct((MAPS, ROWS), F32)),
        in_specs=[SMEM, SMEM] + [VMEM] * 6,
        out_specs=(VMEM,) * 8,
        scratch_shapes=[pltpu.VMEM((ROWS, 512), BF16)],
        compiler_params=vmem(24),
        name="finish",
    )(place, mix_lambda, mine, other, head_gain[None], keep, part, out_weight)
    from_far_a = lax.ppermute(far_a, "x", ring(4, 1))
    from_far_b = lax.ppermute(far_b, "x", ring(4, -1))

    def add(*arrays):
        return sum(a.astype(F32) for a in arrays).astype(BF16)

    low = lax.ppermute(jnp.concatenate([add(up_a, from_far_a), up_b], axis=0), "x", ring(4, 1))
    high = lax.ppermute(jnp.concatenate([down_a, add(down_b, from_far_b)], axis=0), "x", ring(4, -1))
    mixed = add(own, low, high)
    return mixed, jnp.transpose(logs.reshape(4, 2, ROWS), (1, 0, 2))


def solution(mesh):
    fine = Mesh(mesh.devices.reshape(8, 4, 2, 4), ("z", "y", "c", "x"))
    sp = ("z", "y", "c")
    in_specs = (
        P((*sp, "x"), None),
        P(),
        P(None, "x", None),
        P(None, "x", None),
        P(None, "x", None),
        P("x"),
        P(),
        P(None, "x", None),
        P("x", None, None),
        P("x", None),
        P(None, None, "x"),
        P("x", None),
    )
    out_specs = (P((*sp, "x"), None), P(None, "x", sp))
    return jax.shard_map(local, mesh=fine, in_specs=in_specs, out_specs=out_specs, check_vma=False)
```

```python
import functools
import math

import jax
import jax.numpy as jnp
from jax import lax
from jax.experimental import pallas as pl
from jax.experimental.pallas import tpu as pltpu
from jax.sharding import Mesh
from jax.sharding import PartitionSpec as P


NORM_EPS = 1e-06
WINDOW = 16
ROWS = 256
HALF = 128
MAPS = 8
ST = 152
NEG = -1e30
LIMIT = 64.0
LOG2E = math.log2(math.e)
VMEM = pl.BlockSpec(memory_space=pltpu.VMEM)
SMEM = pl.BlockSpec(memory_space=pltpu.SMEM)
F32 = jnp.float32
BF16 = jnp.bfloat16


def vmem(mib):
    return pltpu.CompilerParams(vmem_limit_bytes=mib << 20)


def ring(size, step):
    return [(i, (i + step) % size) for i in range(size)]


def dot(a, b):
    return jnp.dot(a, b, preferred_element_type=F32)


def with_ones(v0, v1):
    values = jnp.concatenate([v0, v1], axis=1)
    return jnp.concatenate([values, jnp.ones((16, values.shape[1]), BF16)], axis=0)


def first_kernel(place_ref, kv_ref, oth_kv_ref, q_own_ref, q_oth_ref, own_ref, oth_ref, q_ref, p_a, p_b):
    for i in range(MAPS):
        here, there = slice(i % 2 * 64, i % 2 * 64 + 64), slice(64 - i % 2 * 64, 128 - i % 2 * 64)
        q_ref[i, here, :ROWS] = q_own_ref[i * 64 : i * 64 + 64]
        q_ref[i, here, ROWS:] = q_oth_ref[i * 64 : i * 64 + 64]
        q_ref[i, there] = jnp.zeros((64, 2 * ROWS), BF16)
    keys = jnp.concatenate([kv_ref[0, 0, :, :HALF], kv_ref[0, 1, :, :HALF]], axis=0)
    oth_keys = jnp.concatenate([oth_kv_ref[0, 0, :, :HALF], oth_kv_ref[0, 1, :, :HALF]], axis=0)
    values = with_ones(kv_ref[0, 0, :, HALF:], kv_ref[0, 1, :, HALF:])
    row = lax.broadcasted_iota(jnp.int32, (ROWS, 2 * ROWS), 0)
    col = lax.broadcasted_iota(jnp.int32, (ROWS, 2 * ROWS), 1)
    seen = row <= jnp.where(col < ROWS, col, jnp.where(place_ref[2] == 0, ROWS, -1))
    diagonal = (row <= col)[:, :ROWS]
    probs = (p_a, p_b)

    def scores(i, slot):
        s = jnp.where(seen, dot(keys, q_ref[i]), NEG)
        seed = jnp.max(jnp.where(diagonal, dot(oth_keys, q_ref[i, :, ROWS:]), NEG), axis=0, keepdims=True)
        top = jnp.max(s, axis=0, keepdims=True)
        top = jnp.concatenate([top[:, :ROWS], jnp.maximum(top[:, ROWS:], seed)], axis=1)
        probs[slot][...] = jnp.exp2(s - top).astype(BF16)
        own_ref[i, 144:152] = jnp.broadcast_to(top[:, :ROWS], (8, ROWS))
        oth_ref[i, 144:152] = jnp.broadcast_to(top[:, ROWS:], (8, ROWS))

    def sums(i, slot):
        out = dot(values, probs[slot][...])
        own_ref[i, 0:144] = out[:, :ROWS]
        oth_ref[i, 0:144] = out[:, ROWS:]

    def two_maps(h, carry):
        scores(2 * h, 0)
        scores(2 * h + 1, 1)
        sums(2 * h, 0)
        sums(2 * h + 1, 1)
        return carry

    lax.fori_loop(0, MAPS // 2, two_maps, 0)


def join_kernel(a, b, c, d, out_ref):
    for i, ref in enumerate((a, b, c, d)):
        out_ref[i] = ref[0]


def split_kernel(rows_ref, a_ref, b_ref):
    a_ref[...] = rows_ref[:32]
    b_ref[...] = rows_ref[32:]


def weights_kernel(key_ref, value_ref, out_ref):
    out_ref[:, :HALF] = key_ref[...]
    out_ref[:, HALF:] = value_ref[...]


def front_kernel(place_ref, p0a, p0b, p1a, p1b, p2a, p2b, p3a, p3b, gain_ref, w_ref, normed_ref, kv_ref):
    x = place_ref[3]

    def put(piece_ref, back, half):
        values = piece_ref[...].astype(F32)
        scale = lax.rsqrt(jnp.mean(values * values, axis=1, keepdims=True) + NORM_EPS)
        at = pl.multiple_of(((x - back) & 3) * 64 + half * 32, 32)
        normed_ref[pl.ds(at, 32), :] = (values * scale * gain_ref[...]).astype(BF16)

    put(p0a, 0, 0)
    put(p0b, 0, 1)
    put(p1a, 1, 0)
    put(p1b, 1, 1)
    put(p3a, 3, 0)
    put(p3b, 3, 1)
    put(p2a, 2, 0)
    put(p2b, 2, 1)
    both = dot(normed_ref[...], w_ref[...])
    values_t = both[:, HALF:].T.astype(BF16)
    for half in range(2):
        rows = slice(half * HALF, half * HALF + HALF)
        kv_ref[0, half, :, :HALF] = both[rows, :HALF].astype(BF16)
        kv_ref[0, half, :, HALF:] = values_t[:, rows]


def chunk_kernel(plan, n_in, rolled, *refs):
    place_ref, q_ref = refs[0], refs[1]
    ins = refs[2 : 2 + n_in]
    own_in, oth_in, own_ref, oth_ref, keys_ref, values_ref, p_a, p_b, over_ref, list_ref = refs[2 + n_in :]
    probs = (p_a, p_b)
    z, y = place_ref[0], place_ref[1]
    visible = jnp.int32(0)
    at = 0
    for _, offsets in plan:
        for dz, dy in offsets:
            sees = ((z + dz) & 7) * 4 + ((y + dy) & 3) < z * 4 + y
            list_ref[visible] = at
            visible = visible + sees.astype(jnp.int32)
            at += 1

    def fetch(which, slot):
        at = 0
        rows = slice(slot * ROWS, slot * ROWS + HALF), slice(slot * ROWS + HALF, slot * ROWS + ROWS)
        for pair, offsets in plan:
            count = len(offsets)

            @pl.when((which >= at) & (which < at + count))
            def _(pair=pair, at=at):
                b = which - at
                for half in range(2):
                    source = ins[pair].at[b, half]
                    keys_ref[rows[half]] = source[:, :HALF]
                    values_ref[0:HALF, rows[half]] = source[:, HALF:]

            at += count

    def keep_state():
        own_ref[...] = own_in[...]
        oth_ref[...] = oth_in[...]

    pl.when(visible == 0)(keep_state)

    @pl.when(visible > 0)
    def _():
        own_ref[:, 144:] = own_in[:, 144:]
        oth_ref[:, 144:] = oth_in[:, 144:]
        over_ref[...] = jnp.full(over_ref.shape, NEG, F32)
        values_ref[HALF:144] = jnp.ones((16, 2 * ROWS), BF16)

        def two_blocks(t, carry):
            fetch(list_ref[2 * t], 0)
            second = 2 * t + 1 < visible
            fetch(list_ref[jnp.minimum(2 * t + 1, visible - 1)], 1)

            @pl.when(jnp.logical_not(second))
            def _():
                values_ref[:, ROWS:] = jnp.zeros((144, ROWS), BF16)

            keys, values = keys_ref[...], values_ref[...]

            def scores(i, slot):
                top = jnp.concatenate([own_in[i, 144:145], oth_in[i, 144:145]], axis=1)
                s = dot(keys, q_ref[i]) - top
                over_ref[i] = jnp.maximum(over_ref[i], jnp.max(s.reshape(-1, 8, 2 * ROWS), axis=0))
                probs[slot][...] = jnp.exp2(s).astype(BF16)

            def sums(i, slot):
                out = dot(values, probs[slot][...])
                own_ref[i, 0:144] = jnp.where(t == 0, own_in[i, 0:144], own_ref[i, 0:144]) + out[:, :ROWS]
                oth_ref[i, 0:144] = jnp.where(t == 0, oth_in[i, 0:144], oth_ref[i, 0:144]) + out[:, ROWS:]

            def two_maps(h, carry):
                scores(2 * h, 0)
                scores(2 * h + 1, 1)
                sums(2 * h, 0)
                sums(2 * h + 1, 1)
                return carry

            if rolled:
                return lax.fori_loop(0, MAPS // 2, two_maps, carry)
            scores(0, 0)
            for i in range(MAPS):
                if i + 1 < MAPS:
                    scores(i + 1, (i + 1) % 2)
                sums(i, i % 2)
            return carry

        lax.fori_loop(0, (visible + 1) // 2, two_blocks, 0)

        @pl.when(jnp.logical_not(jnp.max(over_ref[...]) <= LIMIT))
        def _():
            keep_state()
            values_ref[HALF:144] = jnp.ones((16, 2 * ROWS), BF16)

            def one_block(t, carry):
                fetch(list_ref[t], 0)

                def one_map(i, carry):
                    before = jnp.concatenate([own_ref[i, 144:145], oth_ref[i, 144:145]], axis=1)
                    s = dot(keys_ref[:ROWS], q_ref[i])
                    top = jnp.maximum(before, jnp.max(s, axis=0, keepdims=True))
                    scale = jnp.exp2(before - top)
                    out = dot(values_ref[:, :ROWS], jnp.exp2(s - top).astype(BF16))
                    top8 = jnp.broadcast_to(top, (8, 2 * ROWS))
                    own_ref[i, 0:144] = own_ref[i, 0:144] * scale[:, :ROWS] + out[:, :ROWS]
                    oth_ref[i, 0:144] = oth_ref[i, 0:144] * scale[:, ROWS:] + out[:, ROWS:]
                    own_ref[i, 144:152] = top8[:, :ROWS]
                    oth_ref[i, 144:152] = top8[:, ROWS:]
                    return carry

                return lax.fori_loop(0, MAPS, one_map, carry)

            lax.fori_loop(0, visible, one_block, 0)


STATE = (pltpu.VMEM((MAPS, ST, ROWS), F32), pltpu.VMEM((MAPS, ST, ROWS), F32))


def in_vmem(array):
    return pltpu.with_memory_space_constraint(array, pltpu.VMEM)


def attend_chunk(place, q, state, plan, arrays, rolled=False):
    n = len(arrays)
    blocks = sum(len(offsets) for _, offsets in plan)
    return pl.pallas_call(
        functools.partial(chunk_kernel, plan, n, rolled),
        out_shape=STATE,
        in_specs=[SMEM, VMEM] + [VMEM] * n + [VMEM, VMEM],
        out_specs=(VMEM, VMEM),
        scratch_shapes=[
            pltpu.VMEM((2 * ROWS, HALF), BF16),
            pltpu.VMEM((144, 2 * ROWS), BF16),
            pltpu.VMEM((2 * ROWS, 2 * ROWS), BF16),
            pltpu.VMEM((2 * ROWS, 2 * ROWS), BF16),
            pltpu.VMEM((MAPS, 8, 2 * ROWS), F32),
            pltpu.SMEM((blocks + 1,), jnp.int32),
        ],
        cost_estimate=pl.CostEstimate(
            flops=blocks * MAPS * 2 * 256 * 512 * 512, transcendentals=blocks * MAPS * 256 * 512, bytes_accessed=1 << 20
        ),
        compiler_params=vmem(20),
    )(place, in_vmem(q), *arrays, in_vmem(state[0]), in_vmem(state[1]))


def pool_kernel(place_ref, pool_ref, rim_ref, gate_ref, mix_ref, scale_ref, keep_ref, part_ref):
    span = jnp.left_shift(jnp.int32(2), place_ref[3])
    start = ((place_ref[0] * 4 + place_ref[1]) * 2 + place_ref[2]) * ROWS
    now = pool_ref[...].astype(F32)
    sums = jnp.concatenate([rim_ref[...].astype(F32), now], axis=0)
    rows = WINDOW + ROWS
    picked = jnp.zeros((ROWS, now.shape[1]), F32)
    for width in (1, 2, 4, 8):
        sums = sums + jnp.concatenate([jnp.zeros((width, now.shape[1]), F32), sums[: rows - width]], axis=0)
        picked = jnp.where(span == 2 * width, sums[WINDOW:], picked)
    position = start + lax.broadcasted_iota(jnp.int32, (ROWS, 1), 0)
    counts = jnp.minimum(position + 1, span).astype(F32)
    pooled = (picked / counts - now).astype(BF16)
    mixed = dot(pooled, mix_ref[...]) * scale_ref[...]
    width = now.shape[1]
    keep_ref[...] = jax.nn.sigmoid(gate_ref[:, :width].astype(F32))
    part_ref[...] = jax.nn.sigmoid(gate_ref[:, width:].astype(F32)) * mixed


def finish_kernel(place_ref, lam_ref, a_ref, b_ref, gain_ref, keep_ref, part_ref, w_ref, *refs):
    own_out, up_a, up_b, far_a, far_b, down_a, down_b, log_ref, merged_ref = refs
    x = place_ref[3]
    for h in range(MAPS // 2):
        maps = []
        for m in range(2):
            i = 2 * h + m
            top_a, top_b = a_ref[i, 144:145], b_ref[i, 144:145]
            top = jnp.maximum(top_a, top_b)
            wa, wb = jnp.exp2(top_a - top), jnp.exp2(top_b - top)
            total = a_ref[i, 128:129] * wa + b_ref[i, 128:129] * wb
            log_ref[i : i + 1, :] = (top + jnp.log2(total)) * (1.0 / LOG2E)
            maps.append((a_ref[i, 0:128] * wa + b_ref[i, 0:128] * wb) / total)
        head = maps[0] - lam_ref[h] * maps[1]
        head = head * lax.rsqrt(jnp.mean(head * head, axis=0, keepdims=True) + NORM_EPS)
        cols = slice(h * 128, h * 128 + 128)
        merged = (keep_ref[:, cols] * (head.T * gain_ref[...]) + part_ref[:, cols]).astype(BF16)
        for j in range(4):
            at = pl.multiple_of(((j - x) & 3) * 64, 64)
            merged_ref[pl.ds(at, 64), cols] = merged[j * 64 : j * 64 + 64]
    out = dot(merged_ref[...], w_ref[...]).astype(BF16)
    own_out[...] = out[:64]
    for i, ref in enumerate((up_a, up_b, far_a, far_b, down_a, down_b)):
        ref[...] = out[64 + i * 32 : 96 + i * 32]


def local(tokens, norm_gain, query_weight, key_weight, value_weight, mix_lambda, head_gain, pool_weight, pool_mix, pool_scale, gate_weight, out_weight):
    width = tokens.shape[1]
    z, y, c = lax.axis_index("z"), lax.axis_index("y"), lax.axis_index("c")
    place = jnp.stack([z, y, c, lax.axis_index("x")])
    halves = pl.pallas_call(
        split_kernel,
        out_shape=(pltpu.VMEM((32, width), BF16),) * 2,
        in_specs=[VMEM],
        out_specs=(VMEM, VMEM),
        compiler_params=vmem(4),
        name="split",
    )(tokens)
    up_a = lax.ppermute(halves[0], "x", ring(4, 1))
    down_b = lax.ppermute(halves[1], "x", ring(4, -1))
    up_b = lax.ppermute(halves[1], "x", ring(4, 1))
    down_a = lax.ppermute(halves[0], "x", ring(4, -1))
    far_a = lax.ppermute(up_a, "x", ring(4, 1))
    far_b = lax.ppermute(down_b, "x", ring(4, -1))
    kv_w = pl.pallas_call(
        weights_kernel,
        out_shape=pltpu.VMEM((width, 2 * HALF), BF16),
        in_specs=[VMEM] * 2,
        out_specs=VMEM,
        compiler_params=vmem(6),
        name="weights",
    )(key_weight[:, 0], value_weight[:, 0])
    normed, kv = pl.pallas_call(
        front_kernel,
        out_shape=(jax.ShapeDtypeStruct((ROWS, width), BF16), jax.ShapeDtypeStruct((1, 2, HALF, 2 * HALF), BF16)),
        in_specs=[SMEM] + [VMEM] * 10,
        out_specs=(VMEM, VMEM),
        compiler_params=vmem(16),
        name="front",
    )(place, *map(in_vmem, (*halves, up_a, up_b, far_a, far_b, down_a, down_b)), norm_gain[None], in_vmem(kv_w))
    kv_oth = lax.ppermute(kv, "c", [(0, 1), (1, 0)])

    beside = []
    for step in (1, -1, 2):
        beside.append(lax.ppermute(kv, "y", ring(4, step)))
    group = pl.pallas_call(
        join_kernel,
        out_shape=jax.ShapeDtypeStruct((4, 2, HALF, 2 * HALF), BF16),
        in_specs=[VMEM] * 4,
        out_specs=VMEM,
        compiler_params=vmem(8),
        name="join",
    )(kv, *beside)
    columns = (0, -1, 1, 2)
    up, down = [group], [group]
    for k in range(3):
        up.append(lax.ppermute(up[-1], "z", ring(8, 1)))
        down.append(lax.ppermute(down[-1], "z", ring(8, -1)))
    up.append(lax.ppermute(up[3][:2], "z", ring(8, 1)))
    down.append(lax.ppermute(down[3][2:], "z", ring(8, -1)))

    scale = (query_weight.shape[2] // 2) ** -0.5 * LOG2E
    query_w = query_weight.reshape(width, -1)
    q_own = (
        lax.dot_general(query_w, normed, (((0,), (1,)), ((), ())), preferred_element_type=F32) * scale
    ).astype(BF16)
    q_oth = lax.ppermute(q_own, "c", [(0, 1), (1, 0)])

    pool_in = dot(normed, pool_weight[:, 0]).astype(BF16)
    rim = lax.ppermute(pool_in[ROWS - WINDOW :], ("z", "y", "c"), [(i, i + 1) for i in range(63)])
    gate_weight, pool_in = lax.optimization_barrier((gate_weight, pool_in))
    gate_w = gate_weight.reshape(width, -1)
    q_own, gate_w = lax.optimization_barrier((q_own, gate_w))

    *state, q = pl.pallas_call(
        first_kernel,
        out_shape=(*STATE, pltpu.VMEM((MAPS, 128, 2 * ROWS), BF16)),
        in_specs=[SMEM] + [VMEM] * 4,
        out_specs=(VMEM, VMEM, VMEM),
        scratch_shapes=[pltpu.VMEM((ROWS, 2 * ROWS), BF16)] * 2,
        compiler_params=vmem(16),
        name="first",
    )(place, kv, kv_oth, q_own, q_oth)
    plan = tuple((i, ((0, dy),)) for i, dy in enumerate(columns[1:]))
    state = attend_chunk(place, q, state, plan, beside, rolled=True)
    for k in range(1, 5):
        plan = (
            (0, tuple((-k, dy) for dy in (columns if k < 4 else columns[:2]))),
            (1, tuple((k, dy) for dy in (columns if k < 4 else columns[2:]))),
        )
        state = attend_chunk(place, q, state, plan, (up[k], down[k]))
    other = lax.ppermute(state[1], "c", [(0, 1), (1, 0)])
    normed, mine = lax.optimization_barrier((normed, state[0]))
    gate_pre = dot(normed, gate_w).astype(BF16)
    part_shape = jax.ShapeDtypeStruct((ROWS, 512), F32)
    keep, part = pl.pallas_call(
        pool_kernel,
        out_shape=(part_shape, part_shape),
        in_specs=[SMEM] + [VMEM] * 5,
        out_specs=(VMEM, VMEM),
        compiler_params=vmem(16),
        name="pool",
    )(place, pool_in, rim, gate_pre, pool_mix[0], pool_scale)
    piece = jax.ShapeDtypeStruct((32, width), BF16)
    own, up_a, up_b, far_a, far_b, down_a, down_b, logs = pl.pallas_call(
        finish_kernel,
        out_shape=(jax.ShapeDtypeStruct((64, width), BF16), *[piece] * 6, jax.ShapeDtypeStruct((MAPS, ROWS), F32)),
        in_specs=[SMEM, SMEM] + [VMEM] * 6,
        out_specs=(VMEM,) * 8,
        scratch_shapes=[pltpu.VMEM((ROWS, 512), BF16)],
        compiler_params=vmem(24),
        name="finish",
    )(place, mix_lambda, mine, other, head_gain[None], keep, part, out_weight)
    from_far_a = lax.ppermute(far_a, "x", ring(4, 1))
    from_far_b = lax.ppermute(far_b, "x", ring(4, -1))

    def add(*arrays):
        return sum(a.astype(F32) for a in arrays).astype(BF16)

    low = lax.ppermute(jnp.concatenate([add(up_a, from_far_a), up_b], axis=0), "x", ring(4, 1))
    high = lax.ppermute(jnp.concatenate([down_a, add(down_b, from_far_b)], axis=0), "x", ring(4, -1))
    mixed = add(own, low, high)
    return mixed, jnp.transpose(logs.reshape(4, 2, ROWS), (1, 0, 2))


def solution(mesh):
    fine = Mesh(mesh.devices.reshape(8, 4, 2, 4), ("z", "y", "c", "x"))
    sp = ("z", "y", "c")
    in_specs = (
        P((*sp, "x"), None),
        P(),
        P(None, "x", None),
        P(None, "x", None),
        P(None, "x", None),
        P("x"),
        P(),
        P(None, "x", None),
        P("x", None, None),
        P("x", None),
        P(None, None, "x"),
        P("x", None),
    )
    out_specs = (P((*sp, "x"), None), P(None, "x", sp))
    return jax.shard_map(local, mesh=fine, in_specs=in_specs, out_specs=out_specs, check_vma=False)
```

```python
import functools
import math

import jax
import jax.numpy as jnp
from jax import lax
from jax.experimental import pallas as pl
from jax.experimental.pallas import tpu as pltpu
from jax.sharding import Mesh
from jax.sharding import PartitionSpec as P


NORM_EPS = 1e-06
WINDOW = 16
ROWS = 256
HALF = 128
MAPS = 8
ST = 152
NEG = -1e30
LIMIT = 64.0
LOG2E = math.log2(math.e)
VMEM = pl.BlockSpec(memory_space=pltpu.VMEM)
SMEM = pl.BlockSpec(memory_space=pltpu.SMEM)
F32 = jnp.float32
BF16 = jnp.bfloat16


def vmem(mib):
    return pltpu.CompilerParams(vmem_limit_bytes=mib << 20)


def ring(size, step):
    return [(i, (i + step) % size) for i in range(size)]


def dot(a, b):
    return jnp.dot(a, b, preferred_element_type=F32)


def with_ones(v0, v1):
    values = jnp.concatenate([v0, v1], axis=1)
    return jnp.concatenate([values, jnp.ones((16, values.shape[1]), BF16)], axis=0)


def first_kernel(place_ref, kv_ref, oth_kv_ref, q_own_ref, q_oth_ref, own_ref, oth_ref, q_ref, p_a, p_b):
    for i in range(MAPS):
        here, there = slice(i % 2 * 64, i % 2 * 64 + 64), slice(64 - i % 2 * 64, 128 - i % 2 * 64)
        q_ref[i, here, :ROWS] = q_own_ref[i * 64 : i * 64 + 64]
        q_ref[i, here, ROWS:] = q_oth_ref[i * 64 : i * 64 + 64]
        q_ref[i, there] = jnp.zeros((64, 2 * ROWS), BF16)
    keys = jnp.concatenate([kv_ref[0, 0, :, :HALF], kv_ref[0, 1, :, :HALF]], axis=0)
    oth_keys = jnp.concatenate([oth_kv_ref[0, 0, :, :HALF], oth_kv_ref[0, 1, :, :HALF]], axis=0)
    values = with_ones(kv_ref[0, 0, :, HALF:], kv_ref[0, 1, :, HALF:])
    row = lax.broadcasted_iota(jnp.int32, (ROWS, 2 * ROWS), 0)
    col = lax.broadcasted_iota(jnp.int32, (ROWS, 2 * ROWS), 1)
    seen = row <= jnp.where(col < ROWS, col, jnp.where(place_ref[2] == 0, ROWS, -1))
    diagonal = (row <= col)[:, :ROWS]
    probs = (p_a, p_b)

    def scores(i, slot):
        s = jnp.where(seen, dot(keys, q_ref[i]) * LOG2E, NEG)
        seed = jnp.max(jnp.where(diagonal, dot(oth_keys, q_ref[i, :, ROWS:]) * LOG2E, NEG), axis=0, keepdims=True)
        top = jnp.max(s, axis=0, keepdims=True)
        top = jnp.concatenate([top[:, :ROWS], jnp.maximum(top[:, ROWS:], seed)], axis=1)
        probs[slot][...] = jnp.exp2(s - top).astype(BF16)
        own_ref[i, 144:152] = jnp.broadcast_to(top[:, :ROWS], (8, ROWS))
        oth_ref[i, 144:152] = jnp.broadcast_to(top[:, ROWS:], (8, ROWS))

    def sums(i, slot):
        out = dot(values, probs[slot][...])
        own_ref[i, 0:144] = out[:, :ROWS]
        oth_ref[i, 0:144] = out[:, ROWS:]

    def two_maps(h, carry):
        scores(2 * h, 0)
        scores(2 * h + 1, 1)
        sums(2 * h, 0)
        sums(2 * h + 1, 1)
        return carry

    lax.fori_loop(0, MAPS // 2, two_maps, 0)


def join_kernel(a, b, c, d, out_ref):
    for i, ref in enumerate((a, b, c, d)):
        out_ref[i] = ref[0]


def split_kernel(rows_ref, a_ref, b_ref):
    a_ref[...] = rows_ref[:32]
    b_ref[...] = rows_ref[32:]


def weights_kernel(key_ref, value_ref, out_ref):
    out_ref[:, :HALF] = key_ref[...]
    out_ref[:, HALF:] = value_ref[...]


def front_kernel(place_ref, p0a, p0b, p1a, p1b, p2a, p2b, p3a, p3b, gain_ref, w_ref, normed_ref, kv_ref):
    x = place_ref[3]

    def put(piece_ref, back, half):
        values = piece_ref[...].astype(F32)
        scale = lax.rsqrt(jnp.mean(values * values, axis=1, keepdims=True) + NORM_EPS)
        at = pl.multiple_of(((x - back) & 3) * 64 + half * 32, 32)
        normed_ref[pl.ds(at, 32), :] = (values * scale * gain_ref[...]).astype(BF16)

    put(p0a, 0, 0)
    put(p0b, 0, 1)
    put(p1a, 1, 0)
    put(p1b, 1, 1)
    put(p3a, 3, 0)
    put(p3b, 3, 1)
    put(p2a, 2, 0)
    put(p2b, 2, 1)
    both = dot(normed_ref[...], w_ref[...])
    values_t = both[:, HALF:].T.astype(BF16)
    for half in range(2):
        rows = slice(half * HALF, half * HALF + HALF)
        kv_ref[0, half, :, :HALF] = both[rows, :HALF].astype(BF16)
        kv_ref[0, half, :, HALF:] = values_t[:, rows]


def chunk_kernel(plan, n_in, rolled, *refs):
    place_ref, q_ref = refs[0], refs[1]
    ins = refs[2 : 2 + n_in]
    own_in, oth_in, own_ref, oth_ref, keys_ref, values_ref, p_a, p_b, over_ref, list_ref = refs[2 + n_in :]
    probs = (p_a, p_b)
    z, y = place_ref[0], place_ref[1]
    visible = jnp.int32(0)
    at = 0
    for _, offsets in plan:
        for dz, dy in offsets:
            sees = ((z + dz) & 7) * 4 + ((y + dy) & 3) < z * 4 + y
            list_ref[visible] = at
            visible = visible + sees.astype(jnp.int32)
            at += 1

    def fetch(which, slot):
        at = 0
        rows = slice(slot * ROWS, slot * ROWS + HALF), slice(slot * ROWS + HALF, slot * ROWS + ROWS)
        for pair, offsets in plan:
            count = len(offsets)

            @pl.when((which >= at) & (which < at + count))
            def _(pair=pair, at=at):
                b = which - at
                for half in range(2):
                    source = ins[pair].at[b, half]
                    keys_ref[rows[half]] = source[:, :HALF]
                    values_ref[0:HALF, rows[half]] = source[:, HALF:]

            at += count

    def keep_state():
        def one_map(i, carry):
            own_ref[i] = own_in[i]
            oth_ref[i] = oth_in[i]
            return carry

        lax.fori_loop(0, MAPS, one_map, 0)

    pl.when(visible == 0)(keep_state)

    @pl.when(visible > 0)
    def _():
        own_ref[:, 144:] = own_in[:, 144:]
        oth_ref[:, 144:] = oth_in[:, 144:]
        over_ref[...] = jnp.full(over_ref.shape, NEG, F32)
        values_ref[HALF:144] = jnp.ones((16, 2 * ROWS), BF16)

        def two_blocks(t, carry):
            fetch(list_ref[2 * t], 0)
            second = 2 * t + 1 < visible
            fetch(list_ref[jnp.minimum(2 * t + 1, visible - 1)], 1)

            @pl.when(jnp.logical_not(second))
            def _():
                values_ref[:, ROWS:] = jnp.zeros((144, ROWS), BF16)

            keys, values = keys_ref[...], values_ref[...]

            def scores(i, slot):
                top = jnp.concatenate([own_in[i, 144:145], oth_in[i, 144:145]], axis=1)
                s = dot(keys, q_ref[i]) * LOG2E - top
                over_ref[i] = jnp.maximum(over_ref[i], jnp.max(s.reshape(-1, 8, 2 * ROWS), axis=0))
                probs[slot][...] = jnp.exp2(s).astype(BF16)

            def sums(i, slot):
                out = dot(values, probs[slot][...])
                own_ref[i, 0:144] = jnp.where(t == 0, own_in[i, 0:144], own_ref[i, 0:144]) + out[:, :ROWS]
                oth_ref[i, 0:144] = jnp.where(t == 0, oth_in[i, 0:144], oth_ref[i, 0:144]) + out[:, ROWS:]

            def two_maps(h, carry):
                scores(2 * h, 0)
                scores(2 * h + 1, 1)
                sums(2 * h, 0)
                sums(2 * h + 1, 1)
                return carry

            if rolled:
                return lax.fori_loop(0, MAPS // 2, two_maps, carry)
            scores(0, 0)
            for i in range(MAPS):
                if i + 1 < MAPS:
                    scores(i + 1, (i + 1) % 2)
                sums(i, i % 2)
            return carry

        lax.fori_loop(0, (visible + 1) // 2, two_blocks, 0)

        @pl.when(jnp.logical_not(jnp.max(over_ref[...]) <= LIMIT))
        def _():
            keep_state()
            values_ref[HALF:144] = jnp.ones((16, 2 * ROWS), BF16)

            def one_block(t, carry):
                fetch(list_ref[t], 0)

                def one_map(i, carry):
                    before = jnp.concatenate([own_ref[i, 144:145], oth_ref[i, 144:145]], axis=1)
                    s = dot(keys_ref[:ROWS], q_ref[i]) * LOG2E
                    top = jnp.maximum(before, jnp.max(s, axis=0, keepdims=True))
                    scale = jnp.exp2(before - top)
                    out = dot(values_ref[:, :ROWS], jnp.exp2(s - top).astype(BF16))
                    top8 = jnp.broadcast_to(top, (8, 2 * ROWS))
                    own_ref[i, 0:144] = own_ref[i, 0:144] * scale[:, :ROWS] + out[:, :ROWS]
                    oth_ref[i, 0:144] = oth_ref[i, 0:144] * scale[:, ROWS:] + out[:, ROWS:]
                    own_ref[i, 144:152] = top8[:, :ROWS]
                    oth_ref[i, 144:152] = top8[:, ROWS:]
                    return carry

                return lax.fori_loop(0, MAPS, one_map, carry)

            lax.fori_loop(0, visible, one_block, 0)


STATE = (pltpu.VMEM((MAPS, ST, ROWS), F32), pltpu.VMEM((MAPS, ST, ROWS), F32))


def in_vmem(array):
    return pltpu.with_memory_space_constraint(array, pltpu.VMEM)


def attend_chunk(place, q, state, plan, arrays, rolled=False):
    n = len(arrays)
    blocks = sum(len(offsets) for _, offsets in plan)
    return pl.pallas_call(
        functools.partial(chunk_kernel, plan, n, rolled),
        out_shape=STATE,
        in_specs=[SMEM, VMEM] + [VMEM] * n + [VMEM, VMEM],
        out_specs=(VMEM, VMEM),
        scratch_shapes=[
            pltpu.VMEM((2 * ROWS, HALF), BF16),
            pltpu.VMEM((144, 2 * ROWS), BF16),
            pltpu.VMEM((2 * ROWS, 2 * ROWS), BF16),
            pltpu.VMEM((2 * ROWS, 2 * ROWS), BF16),
            pltpu.VMEM((MAPS, 8, 2 * ROWS), F32),
            pltpu.SMEM((blocks + 1,), jnp.int32),
        ],
        cost_estimate=pl.CostEstimate(
            flops=blocks * MAPS * 2 * 256 * 512 * 512, transcendentals=blocks * MAPS * 256 * 512, bytes_accessed=1 << 20
        ),
        compiler_params=vmem(20),
    )(place, in_vmem(q), *arrays, in_vmem(state[0]), in_vmem(state[1]))


def pool_kernel(place_ref, pool_ref, rim_ref, gate_ref, mix_ref, scale_ref, keep_ref, part_ref):
    span = jnp.left_shift(jnp.int32(2), place_ref[3])
    start = ((place_ref[0] * 4 + place_ref[1]) * 2 + place_ref[2]) * ROWS
    now = pool_ref[...].astype(F32)
    sums = jnp.concatenate([rim_ref[...].astype(F32), now], axis=0)
    rows = WINDOW + ROWS
    picked = jnp.zeros((ROWS, now.shape[1]), F32)
    for width in (1, 2, 4, 8):
        sums = sums + jnp.concatenate([jnp.zeros((width, now.shape[1]), F32), sums[: rows - width]], axis=0)
        picked = jnp.where(span == 2 * width, sums[WINDOW:], picked)
    position = start + lax.broadcasted_iota(jnp.int32, (ROWS, 1), 0)
    counts = jnp.minimum(position + 1, span).astype(F32)
    pooled = (picked / counts - now).astype(BF16)
    mixed = dot(pooled, mix_ref[...]) * scale_ref[...]
    width = now.shape[1]
    keep_ref[...] = jax.nn.sigmoid(gate_ref[:, :width].astype(F32))
    part_ref[...] = jax.nn.sigmoid(gate_ref[:, width:].astype(F32)) * mixed


def finish_kernel(place_ref, lam_ref, a_ref, b_ref, gain_ref, keep_ref, part_ref, w_ref, *refs):
    own_out, up_a, up_b, far_a, far_b, down_a, down_b, log_ref, merged_ref = refs
    x = place_ref[3]
    for h in range(MAPS // 2):
        maps = []
        for m in range(2):
            i = 2 * h + m
            top_a, top_b = a_ref[i, 144:145], b_ref[i, 144:145]
            top = jnp.maximum(top_a, top_b)
            wa, wb = jnp.exp2(top_a - top), jnp.exp2(top_b - top)
            total = a_ref[i, 128:129] * wa + b_ref[i, 128:129] * wb
            log_ref[i : i + 1, :] = (top + jnp.log2(total)) * (1.0 / LOG2E)
            maps.append((a_ref[i, 0:128] * wa + b_ref[i, 0:128] * wb) / total)
        head = maps[0] - lam_ref[h] * maps[1]
        head = head * lax.rsqrt(jnp.mean(head * head, axis=0, keepdims=True) + NORM_EPS)
        cols = slice(h * 128, h * 128 + 128)
        merged = (keep_ref[:, cols] * (head.T * gain_ref[...]) + part_ref[:, cols]).astype(BF16)
        for j in range(4):
            at = pl.multiple_of(((j - x) & 3) * 64, 64)
            merged_ref[pl.ds(at, 64), cols] = merged[j * 64 : j * 64 + 64]
    out = dot(merged_ref[...], w_ref[...]).astype(BF16)
    own_out[...] = out[:64]
    for i, ref in enumerate((up_a, up_b, far_a, far_b, down_a, down_b)):
        ref[...] = out[64 + i * 32 : 96 + i * 32]


def local(tokens, norm_gain, query_weight, key_weight, value_weight, mix_lambda, head_gain, pool_weight, pool_mix, pool_scale, gate_weight, out_weight):
    width = tokens.shape[1]
    z, y, c = lax.axis_index("z"), lax.axis_index("y"), lax.axis_index("c")
    place = jnp.stack([z, y, c, lax.axis_index("x")])
    halves = pl.pallas_call(
        split_kernel,
        out_shape=(pltpu.VMEM((32, width), BF16),) * 2,
        in_specs=[VMEM],
        out_specs=(VMEM, VMEM),
        compiler_params=vmem(4),
        name="split",
    )(tokens)
    up_a = lax.ppermute(halves[0], "x", ring(4, 1))
    down_b = lax.ppermute(halves[1], "x", ring(4, -1))
    up_b = lax.ppermute(halves[1], "x", ring(4, 1))
    down_a = lax.ppermute(halves[0], "x", ring(4, -1))
    far_a = lax.ppermute(up_a, "x", ring(4, 1))
    far_b = lax.ppermute(down_b, "x", ring(4, -1))
    kv_w = pl.pallas_call(
        weights_kernel,
        out_shape=pltpu.VMEM((width, 2 * HALF), BF16),
        in_specs=[VMEM] * 2,
        out_specs=VMEM,
        compiler_params=vmem(6),
        name="weights",
    )(key_weight[:, 0], value_weight[:, 0])
    normed, kv = pl.pallas_call(
        front_kernel,
        out_shape=(jax.ShapeDtypeStruct((ROWS, width), BF16), jax.ShapeDtypeStruct((1, 2, HALF, 2 * HALF), BF16)),
        in_specs=[SMEM] + [VMEM] * 10,
        out_specs=(VMEM, VMEM),
        compiler_params=vmem(16),
        name="front",
    )(place, *map(in_vmem, (*halves, up_a, up_b, far_a, far_b, down_a, down_b)), norm_gain[None], in_vmem(kv_w))
    kv_oth = lax.ppermute(kv, "c", [(0, 1), (1, 0)])

    beside = []
    for step in (1, -1, 2):
        beside.append(lax.ppermute(kv, "y", ring(4, step)))
    group = pl.pallas_call(
        join_kernel,
        out_shape=jax.ShapeDtypeStruct((4, 2, HALF, 2 * HALF), BF16),
        in_specs=[VMEM] * 4,
        out_specs=VMEM,
        compiler_params=vmem(8),
        name="join",
    )(kv, *beside)
    columns = (0, -1, 1, 2)
    up, down = [group], [group]
    for k in range(3):
        up.append(lax.ppermute(up[-1], "z", ring(8, 1)))
        down.append(lax.ppermute(down[-1], "z", ring(8, -1)))
    up.append(lax.ppermute(up[3][:2], "z", ring(8, 1)))
    down.append(lax.ppermute(down[3][2:], "z", ring(8, -1)))

    scale = (query_weight.shape[2] // 2) ** -0.5
    query_w = query_weight.reshape(width, -1)
    q_own = (
        lax.dot_general(query_w, normed, (((0,), (1,)), ((), ())), preferred_element_type=F32) * scale
    ).astype(BF16)
    q_oth = lax.ppermute(q_own, "c", [(0, 1), (1, 0)])

    pool_in = dot(normed, pool_weight[:, 0]).astype(BF16)
    rim = lax.ppermute(pool_in[ROWS - WINDOW :], ("z", "y", "c"), [(i, i + 1) for i in range(63)])
    gate_weight, pool_in = lax.optimization_barrier((gate_weight, pool_in))
    gate_w = gate_weight.reshape(width, -1)
    q_own, gate_w = lax.optimization_barrier((q_own, gate_w))

    *state, q = pl.pallas_call(
        first_kernel,
        out_shape=(*STATE, pltpu.VMEM((MAPS, 128, 2 * ROWS), BF16)),
        in_specs=[SMEM] + [VMEM] * 4,
        out_specs=(VMEM, VMEM, VMEM),
        scratch_shapes=[pltpu.VMEM((ROWS, 2 * ROWS), BF16)] * 2,
        compiler_params=vmem(16),
        name="first",
    )(place, kv, kv_oth, q_own, q_oth)
    plan = tuple((i, ((0, dy),)) for i, dy in enumerate(columns[1:]))
    state = attend_chunk(place, q, state, plan, beside, rolled=True)
    for k in range(1, 5):
        plan = (
            (0, tuple((-k, dy) for dy in (columns if k < 4 else columns[:2]))),
            (1, tuple((k, dy) for dy in (columns if k < 4 else columns[2:]))),
        )
        state = attend_chunk(place, q, state, plan, (up[k], down[k]))
    other = lax.ppermute(state[1], "c", [(0, 1), (1, 0)])
    normed, mine = lax.optimization_barrier((normed, state[0]))
    gate_pre = dot(normed, gate_w).astype(BF16)
    part_shape = jax.ShapeDtypeStruct((ROWS, 512), F32)
    keep, part = pl.pallas_call(
        pool_kernel,
        out_shape=(part_shape, part_shape),
        in_specs=[SMEM] + [VMEM] * 5,
        out_specs=(VMEM, VMEM),
        compiler_params=vmem(16),
        name="pool",
    )(place, pool_in, rim, gate_pre, pool_mix[0], pool_scale)
    piece = jax.ShapeDtypeStruct((32, width), BF16)
    own, up_a, up_b, far_a, far_b, down_a, down_b, logs = pl.pallas_call(
        finish_kernel,
        out_shape=(jax.ShapeDtypeStruct((64, width), BF16), *[piece] * 6, jax.ShapeDtypeStruct((MAPS, ROWS), F32)),
        in_specs=[SMEM, SMEM] + [VMEM] * 6,
        out_specs=(VMEM,) * 8,
        scratch_shapes=[pltpu.VMEM((ROWS, 512), BF16)],
        compiler_params=vmem(24),
        name="finish",
    )(place, mix_lambda, mine, other, head_gain[None], keep, part, out_weight)
    from_far_a = lax.ppermute(far_a, "x", ring(4, 1))
    from_far_b = lax.ppermute(far_b, "x", ring(4, -1))

    def add(*arrays):
        return sum(a.astype(F32) for a in arrays).astype(BF16)

    low = lax.ppermute(jnp.concatenate([add(up_a, from_far_a), up_b], axis=0), "x", ring(4, 1))
    high = lax.ppermute(jnp.concatenate([down_a, add(down_b, from_far_b)], axis=0), "x", ring(4, -1))
    mixed = add(own, low, high)
    return mixed, jnp.transpose(logs.reshape(4, 2, ROWS), (1, 0, 2))


def solution(mesh):
    fine = Mesh(mesh.devices.reshape(8, 4, 2, 4), ("z", "y", "c", "x"))
    sp = ("z", "y", "c")
    in_specs = (
        P((*sp, "x"), None),
        P(),
        P(None, "x", None),
        P(None, "x", None),
        P(None, "x", None),
        P("x"),
        P(),
        P(None, "x", None),
        P("x", None, None),
        P("x", None),
        P(None, None, "x"),
        P("x", None),
    )
    out_specs = (P((*sp, "x"), None), P(None, "x", sp))
    return jax.shard_map(local, mesh=fine, in_specs=in_specs, out_specs=out_specs, check_vma=False)
```
